32 devices in a mesh: ep: 8 (over z, y), tp: 4 (over x, core).
Axes of the slice: x: 2, y: 2, z: 4, core: 2. Of those that a mesh axis runs over, the one named last changes fastest.
Arguments:
- queries: bfloat16 [1024, 512], P('ep', 'tp'), may hold values from -8 to 8
- key_cache: bfloat16 [4, 64, 1024], P('tp', None, 'ep'), may hold values from -4.5 to 4.5
- value_cache: bfloat16 [4, 64, 1024], P('tp', None, 'ep'), may hold values from -6 to 6
- cum_gate: float32 [4, 1024], P('tp'), may hold values from -256 to 0, as said below
- out_weight: bfloat16 [512, 2048], replicated, may hold values from -1 to 1
- routed_input: bfloat16 [2048, 2048], P('ep'), may hold values from -6 to 6
- norm_gain: bfloat16 [2048], replicated, may hold values from 0.099609375 to 1.8984375
- routes: int32 [2048, 2], P('ep'), may hold values from 0 to 7, all different within a row; in each aligned block of 64 rows (0 to 63, 64 to 127, ...) at most 24 rows name the same one
- route_weight: float32 [2048, 2], P('ep'), may hold values from 0.2 to 1
- expert_gate: bfloat16 [8, 2048, 1024], P('ep', None, 'tp'), may hold values from -0.125 to 0.125
- expert_up: bfloat16 [8, 2048, 1024], P('ep', None, 'tp'), may hold values from -0.125 to 0.125
- expert_down: bfloat16 [8, 1024, 2048], P('ep', 'tp'), may hold values from -0.1875 to 0.1875
Outputs:
- mixed_out: bfloat16 [1024, 2048], P(('ep', 'tp'))
- expert_out: bfloat16 [2048, 2048], P(('ep', 'tp'))
The draws below stay inside these ranges and needn't reach their ends.
Inputs may be any that keep to these rules, and one draw needn't show every extreme that they name: `cum_gate`: Non-increasing along positions in every head. `routes`: each row names 2 different experts. In each aligned block of 64 rows (the rows of one device) no expert is named by more than 24 rows, a bound that some block reaches.
All inputs are finite; a program needn't handle non-finite values.
Results may differ from the reference program's by a relative error of at most 0.012.
Values may be sent and summed in bfloat16 or wider, within the bound.
A program may use at most 64 MiB of HBM per device.

```python
import math
import jax
import jax.numpy as jnp
import numpy as np
from jax import lax

D = 2048
HEADS = 8
HEAD = 64
KV_HEADS = 4
FFE = 1024
TOPK = 2
SEQ_ROWS = 128
TOK_DEV = 64
FIRST_TOKENS = 1024
ROUTED_TOKENS = 2048
EXPERTS = 8
CAP = 24
N_TP = 4


def draw_queries(key, part):
    base_key = jax.random.fold_in(key, 11)
    values = jnp.clip(jax.random.normal(base_key, (FIRST_TOKENS, HEADS * HEAD), jnp.float32), -4.0, 4.0)
    return values.astype(jnp.bfloat16)


def draw_key_cache(key, part):
    base_key = jax.random.fold_in(key, 13)
    values = jnp.clip(jax.random.normal(base_key, (KV_HEADS, HEAD, FIRST_TOKENS), jnp.float32), -4.0, 4.0)
    return values.astype(jnp.bfloat16)


def draw_cum_gate(key, part):
    ordering_random_key, gradual_random_key, quick_random_key, block_random_key, coarse_random_key, spike_random_key, loss_random_key = jax.random.split(jax.random.fold_in(key, 17), 7)
    ranks = jax.random.permutation(ordering_random_key, KV_HEADS)
    gradual_decay = ranks < KV_HEADS // 2
    rough = jax.random.uniform(coarse_random_key, (KV_HEADS, FIRST_TOKENS), jnp.float32, 0.2, 1.8)
    slow_rate = jax.random.uniform(gradual_random_key, (KV_HEADS,), jnp.float32, 0.1, 0.4) / FIRST_TOKENS
    fast_rate = 1.0 / jax.random.uniform(quick_random_key, (KV_HEADS,), jnp.float32, 30.0, 100.0)
    rate = jnp.where(gradual_decay, slow_rate, fast_rate)
    factor = jnp.exp(jax.random.uniform(block_random_key, (FIRST_TOKENS // SEQ_ROWS,), jnp.float32, -0.7, 0.7))
    per_position = jnp.repeat(factor, SEQ_ROWS)
    update_steps = -rate[:, None] * per_position[None, :] * rough
    marked_positions = jax.random.randint(spike_random_key, (2,), 0, FIRST_TOKENS)
    loss_values = jnp.log(jax.random.uniform(loss_random_key, (2,), jnp.float32, 0.5, 0.8))
    sudden_spike = jnp.zeros((FIRST_TOKENS,), jnp.float32).at[marked_positions].add(loss_values)
    update_steps = update_steps + jnp.where(gradual_decay[:, None], sudden_spike[None, :], 0.0)
    return jnp.cumsum(update_steps, axis=1)


def block_scale(stream_key, shape, cuts, low, largest):
    gain, own = 1.0, jax.random.fold_in(stream_key, 6)
    for dim, shards_of in cuts:
        draws = jnp.exp(jax.random.uniform(jax.random.fold_in(own, dim), (shards_of,), jnp.float32, low / len(cuts), largest / len(cuts)))
        gain = gain * jnp.repeat(draws, shape[dim] // shards_of).reshape([-1 if axis == dim else 1 for axis in range(len(shape))])
    return gain


def routed_block(stream_key, own, number, rows, count, top, bound, lean):
    order = jax.random.permutation(stream_key, count)
    packed, usual = load_shares(count, rows * top, bound, lean, True), load_shares(count, rows * top, bound, lean, False)
    places = jnp.arange(count)

    def named(sizes, turn):
        used = int((sizes > 0).sum())
        fixed = max(1, used // 4)
        passed = fixed + (places - fixed + turn * (used - fixed)) % max(1, count - fixed)
        return jnp.zeros((count,), jnp.int32).at[order[jnp.where(places < fixed, places, passed)]].set(jnp.asarray(sizes, jnp.int32))

    sizes = jnp.where(number % 4 == 0, named(packed, number // 4), named(usual, number - number // 4 - 1))
    mixed = jax.random.permutation(jax.random.fold_in(own, 3), count)
    donor, taker = mixed[0:count // 2 * 2:2], mixed[1:count // 2 * 2:2]
    margin = jnp.minimum(sizes[donor] - 1, bound - sizes[taker]) // 2
    margin = jnp.where((donor == order[0]) | (taker == order[0]) | (sizes[taker] == 0), 0, jnp.maximum(margin, 0))
    passed = jax.random.randint(jax.random.fold_in(own, 4), (count // 2,), 0, 1 << 20) % (margin + 1)
    sizes = sizes.at[donor].add(-passed).at[taker].add(passed)
    members = jnp.searchsorted(jnp.cumsum(sizes), jnp.arange(rows * top), side="right").astype(jnp.int32)
    table = members.reshape(top, rows).T
    table = table[jax.random.permutation(jax.random.fold_in(own, 1), rows)]
    turn = jax.random.randint(jax.random.fold_in(own, 2), (rows, 1), 0, top)
    return jnp.take_along_axis(table, (jnp.arange(top)[None, :] + turn) % top, axis=1)


def load_shares(amount, total, bound, slope, full):
    loads = [(1 << 20) // math.isqrt(rank ** slope) + 1 for rank in range(1, amount + 1)]
    largest = bound if full else min(bound, max(-(-total // amount), total * loads[0] // sum(loads)))
    least = 1 if total - largest >= amount - 1 else 0
    counts, spare = [largest] + [least] * (amount - 1), total - largest - least * (amount - 1)
    while spare > 0:
        movable = [i for i in range(1, amount) if counts[i] < largest] or [i for i in range(1, amount) if counts[i] < bound]
        whole, budget = sum([loads[i] for i in movable]), spare
        for i in movable:
            addition = min(bound - counts[i], max(1, budget * loads[i] // whole), spare)
            counts[i] = counts[i] + addition
            spare = spare - addition
    return np.array(counts)


def centred(key, dims, spread, bound, pieces=(), kind=jnp.bfloat16):
    result = jax.random.normal(key, dims, jnp.float32) * spread
    if len(pieces) > 0:
        result = block_scale(key, dims, pieces, -0.22, 0.18) * result
    return jnp.clip(result, min=-bound, max=bound).astype(kind)


def setup_inputs(seed: int = 0) -> dict:
    keys = jax.random.split(jax.random.key(seed), 13)
    queries = draw_queries(jax.random.fold_in(keys[12], 71), 0)
    key_cache = draw_key_cache(jax.random.fold_in(keys[12], 71), 0)
    value_cache = centred(keys[2], (KV_HEADS, HEAD, FIRST_TOKENS), 1.0, 6.0, ((0, 4), (2, 8)))
    cum_gate = draw_cum_gate(jax.random.fold_in(keys[12], 71), 0)
    out_weight = centred(keys[4], (HEADS * HEAD, D), (HEADS * HEAD // 16) ** -0.5, 1.0)
    routed_input = centred(keys[5], (ROUTED_TOKENS, D), 1.0, 6.0, ((0, 8),))
    norm_gain = jnp.clip(1.0 + 0.18 * jax.random.normal(keys[6], (D,), jnp.float32), 0.099609375, 1.8984375).astype(jnp.bfloat16)
    routes_keys = jax.random.split(jax.random.fold_in(keys[7], 1), ROUTED_TOKENS // TOK_DEV)
    routes_turns = jax.random.permutation(jax.random.fold_in(keys[7], 3), ROUTED_TOKENS // TOK_DEV)
    routes = jax.vmap(lambda own, number: routed_block(jax.random.fold_in(keys[7], 2), own, number, TOK_DEV, EXPERTS, TOPK, CAP, 1))(routes_keys, routes_turns).reshape((ROUTED_TOKENS, TOPK))
    route_weight = jnp.clip(0.2 + 0.8 * jax.random.uniform(keys[8], (ROUTED_TOKENS, TOPK), jnp.float32) ** block_scale(keys[8], (ROUTED_TOKENS, TOPK), ((0, 8),), -0.2, 0.2), 0.2, 1.0)
    expert_gate = centred(keys[9], (EXPERTS, D, FFE), D ** -0.5, 0.125, ((0, 8), (2, 4)))
    expert_up = centred(keys[10], (EXPERTS, D, FFE), D ** -0.5, 0.125, ((0, 8), (2, 4)))
    expert_down = centred(keys[11], (EXPERTS, FFE, D), FFE ** -0.5, 0.1875, ((0, 8), (1, 4)))
    return dict(queries=queries, key_cache=key_cache, value_cache=value_cache, cum_gate=cum_gate, out_weight=out_weight, routed_input=routed_input, norm_gain=norm_gain, routes=routes, route_weight=route_weight, expert_gate=expert_gate, expert_up=expert_up, expert_down=expert_down)


def attend_block(query_block, keys_head, values_head, gate_head, block_start):
    rows_here = query_block.shape[0]
    scores = jnp.einsum('tgd,ds->tgs', query_block, keys_head) * HEAD ** (-0.5)
    query_pos = block_start + jnp.arange(rows_here, dtype=jnp.int32)
    gate_query = lax.dynamic_slice_in_dim(gate_head, block_start, rows_here, 0)
    scores = scores + gate_query[:, None, None] - gate_head[None, None, :]
    key_pos = jnp.arange(FIRST_TOKENS, dtype=jnp.int32)
    allowed = key_pos[None, :] <= query_pos[:, None]
    scores = jnp.where(allowed[:, None, :], scores, -jnp.inf)
    highest = lax.optimization_barrier(jnp.max(scores, axis=-1, keepdims=True))
    weights = jnp.exp(scores - highest)
    total = lax.optimization_barrier(jnp.sum(weights, axis=-1))
    rounded = lax.optimization_barrier(weights.astype(jnp.bfloat16)).astype(jnp.float32)
    summed = jnp.einsum('tgs,ds->tgd', rounded, values_head)
    return (summed / total[..., None]).astype(jnp.bfloat16)

def reference(queries, key_cache, value_cache, cum_gate, out_weight, routed_input, norm_gain, routes, route_weight, expert_gate, expert_up, expert_down):
    group = HEADS // KV_HEADS
    nblocks = FIRST_TOKENS // SEQ_ROWS
    query_all = queries.astype(jnp.float32).reshape(nblocks, SEQ_ROWS, KV_HEADS, group, HEAD)
    keys_all = key_cache.astype(jnp.float32)
    values_all = value_cache.astype(jnp.float32)

    def one_pair(index):
        block = index // KV_HEADS
        head = index % KV_HEADS
        query_block = query_all[block, :, head]
        start = (block * SEQ_ROWS).astype(jnp.int32)
        return attend_block(query_block, keys_all[head], values_all[head], cum_gate[head], start)
    attended = lax.map(one_pair, jnp.arange(nblocks * KV_HEADS, dtype=jnp.int32))
    attended = attended.reshape(nblocks, KV_HEADS, SEQ_ROWS, group, HEAD).transpose(0, 2, 1, 3, 4).reshape(FIRST_TOKENS, HEADS * HEAD)
    mixed_out = jnp.dot(attended, out_weight, preferred_element_type=jnp.float32).astype(jnp.bfloat16)
    source = routed_input.astype(jnp.float32)
    scale = lax.rsqrt(lax.optimization_barrier(jnp.mean(source * source, axis=-1, keepdims=True)) + 1e-06)
    normed = (source * scale * norm_gain.astype(jnp.float32)).astype(jnp.bfloat16)
    nparts = ROUTED_TOKENS // TOK_DEV
    slots_all = EXPERTS * CAP
    pairs = routes.reshape(nparts, TOK_DEV * TOPK)
    same = (pairs[:, :, None] == jnp.arange(EXPERTS, dtype=jnp.int32)[None, None, :]).astype(jnp.int32)
    earlier = jnp.cumsum(same, axis=1) - same
    rank = lax.optimization_barrier(jnp.sum(earlier * same, axis=2))
    slot = pairs * CAP + rank
    chooser = (slot[:, :, None] == jnp.arange(slots_all, dtype=jnp.int32)[None, None, :]).astype(jnp.float32)
    chooser = chooser.reshape(nparts, TOK_DEV, TOPK, slots_all)
    normed_blocks = normed.astype(jnp.float32).reshape(nparts, TOK_DEV, D)
    width_part = FFE // N_TP

    def one_expert(expert):
        picks = lax.dynamic_slice_in_dim(chooser, expert * CAP, CAP, 3)
        gathered = jnp.einsum('btkc,btd->bcd', picks, normed_blocks).astype(jnp.bfloat16).reshape(nparts * CAP, D)
        gate = jnp.dot(gathered, expert_gate[expert], preferred_element_type=jnp.float32)
        upper = jnp.dot(gathered, expert_up[expert], preferred_element_type=jnp.float32)
        hidden = (jax.nn.silu(gate) * upper).astype(jnp.bfloat16)
        hidden_parts = hidden.astype(jnp.float32).reshape(nparts * CAP, N_TP, width_part)
        down_parts = expert_down[expert].astype(jnp.float32).reshape(N_TP, width_part, D)
        partial_value = jnp.einsum('rqf,qfd->qrd', hidden_parts, down_parts)
        partial_value = lax.optimization_barrier(partial_value.astype(jnp.bfloat16)).astype(jnp.float32)
        return lax.optimization_barrier(jnp.sum(partial_value, axis=0)).astype(jnp.bfloat16).reshape(nparts, CAP, D)
    results = lax.map(one_expert, jnp.arange(EXPERTS, dtype=jnp.int32))
    rank_blocks = rank.reshape(nparts, TOK_DEV, TOPK)
    expert_blocks = routes.reshape(nparts, TOK_DEV, TOPK)
    block_ids = jnp.arange(nparts, dtype=jnp.int32)[:, None, None]
    picked = results[expert_blocks, block_ids, rank_blocks].astype(jnp.float32)
    mixed_weights = route_weight.reshape(nparts, TOK_DEV, TOPK)[..., None] * picked
    expert_out = lax.optimization_barrier(jnp.sum(mixed_weights, axis=2)).reshape(ROUTED_TOKENS, D).astype(jnp.bfloat16)
    return (mixed_out, expert_out)
```

```python
import functools

import jax
import jax.numpy as jnp
from jax import lax
from jax.experimental import pallas as pl
from jax.experimental.pallas import tpu as pltpu
from jax.sharding import PartitionSpec as P

MESH = pl.DeviceIdType.MESH


def fused_kernel(
    n,
    tpn,
    cap,
    q_ref,
    gate_ref,
    gain_ref,
    routes_ref,
    rw_ref,
    k_any,
    v_any,
    ow_any,
    x_any,
    wg_any,
    wu_any,
    wd_any,
    mixed_ref,
    out_ref,
    xbuf,
    wgv,
    wuv,
    wdv,
    owv,
    kv,
    att,
    attr,
    sel,
    sbuf,
    recv,
    part,
    r1,
    s2,
    r2,
    s3,
    rbuf,
    lsem,
    kvs,
    kvr,
    ats,
    atr,
    a_s,
    a_r,
    bx_s,
    bx_r,
    bc_s,
    bc_r,
    c_s,
    c_r,
    r1_s,
    r1_r,
    r2_s,
    r2_r,
    r3_s,
    r3_r,
):
    e = lax.axis_index("ep")
    t = lax.axis_index("tp")
    partner = t + 1 - 2 * lax.rem(t, 2)
    peer = lax.rem(t + 2, tpn)
    opp = lax.rem(partner + 2, tpn)
    mate = e + 1 - 2 * lax.rem(e, 2)
    half = n // 2
    own_rows, width = xbuf.shape
    wide = width // 2
    head = k_any.shape[1]
    seq = q_ref.shape[0]

    barrier = pltpu.get_barrier_semaphore()
    for s in range(1, n):
        pl.semaphore_signal(
            barrier, inc=1, device_id={"ep": lax.rem(e + s, n), "tp": t}, device_id_type=MESH
        )
    for s in range(1, tpn):
        pl.semaphore_signal(
            barrier, inc=1, device_id={"ep": e, "tp": lax.rem(t + s, tpn)}, device_id_type=MESH
        )

    load_x = pltpu.make_async_copy(x_any.at[pl.ds(t * own_rows, own_rows)], xbuf, lsem.at[0])
    load_k = pltpu.make_async_copy(k_any.at[0], kv.at[e, pl.ds(0, head)], lsem.at[1])
    load_v = pltpu.make_async_copy(v_any.at[0], kv.at[e, pl.ds(head, head)], lsem.at[2])
    load_g = pltpu.make_async_copy(wg_any.at[0], wgv, lsem.at[3])
    load_u = pltpu.make_async_copy(wu_any.at[0], wuv, lsem.at[4])
    load_d = pltpu.make_async_copy(wd_any.at[0], wdv, lsem.at[5])
    load_o = pltpu.make_async_copy(ow_any, owv, lsem.at[6])
    load_k.start()
    load_v.start()
    load_x.start()
    load_g.start()
    load_u.start()
    load_d.start()
    load_o.start()

    def remote(src, dst, ssem, rsem, ep, tp):
        return pltpu.make_async_remote_copy(
            src_ref=src,
            dst_ref=dst,
            send_sem=ssem,
            recv_sem=rsem,
            device_id={"ep": ep, "tp": tp},
            device_id_type=MESH,
        )

    def kv_far(s):
        return remote(kv.at[e], kv.at[e], kvs.at[s], kvr.at[s], lax.rem(e + 2 * s, n), t)

    def kv_far_in(s):
        src = lax.rem(e - 2 * s + n, n)
        return remote(kv.at[src], kv.at[src], kvs.at[s], kvr.at[s], lax.rem(e + 2 * s, n), t)

    def kv_mate(s):
        src = lax.rem(e - 2 * s + n, n)
        return remote(kv.at[src], kv.at[src], kvs.at[half + s], kvr.at[half + s], mate, t)

    def kv_mate_in(s):
        src = lax.rem(mate - 2 * s + n, n)
        return remote(kv.at[src], kv.at[src], kvs.at[half + s], kvr.at[half + s], mate, t)

    def source(s):
        return lax.rem(e - s + n, n)

    def send_a(s):
        dst = lax.rem(e + s, n)
        return remote(sbuf.at[dst], recv.at[e, t], a_s.at[s], a_r.at[s], dst, t)

    def copy_a(s):
        src = source(s)
        return remote(sbuf.at[src], recv.at[src, t], a_s.at[s], a_r.at[s], lax.rem(e + s, n), t)

    def copy_bx(s, col):
        src = source(s)
        return remote(recv.at[src, col], recv.at[src, col], bx_s.at[s], bx_r.at[s], e, peer)

    def copy_bc(s, col):
        src = source(s)
        return remote(recv.at[src, col], recv.at[src, col], bc_s.at[s], bc_r.at[s], e, partner)

    def copy_c(s, col):
        src = source(s)
        return remote(recv.at[src, col], recv.at[src, col], c_s.at[s], c_r.at[s], e, partner)

    def copy_r1(s, which, col):
        src = source(s)
        return remote(
            part.at[src, col], r1.at[src, which], r1_s.at[s, which], r1_r.at[s, which], e, partner
        )

    def copy_r2(s):
        src = source(s)
        return remote(s2.at[src], r2.at[src], r2_s.at[s], r2_r.at[s], e, peer)

    def copy_r3(s):
        src = source(s)
        return remote(s3.at[src], rbuf.at[e], r3_s.at[s], r3_r.at[s], src, t)

    def copy_r3_in(s):
        src = lax.rem(e + s, n)
        return remote(s3.at[src], rbuf.at[src], r3_s.at[s], r3_r.at[s], source(s), t)

    load_k.wait()
    load_v.wait()
    pl.semaphore_wait(barrier, n - 1 + tpn - 1)
    for s in range(1, half):
        kv_far(s).start()
    kv_mate(0).start()

    lanes = 2 * n * cap
    place = lax.broadcasted_iota(jnp.int32, (own_rows, lanes), 1).astype(jnp.float32) + 0.5
    expert = jnp.floor(place / (2.0 * cap))
    inside = place - 0.5 - expert * (2.0 * cap)
    right = inside >= cap
    slot = jnp.where(right, inside - cap, inside)
    rows = routes_ref[pl.ds(pl.multiple_of(t * own_rows, own_rows), own_rows), :].astype(jnp.float32)
    top = rows.shape[1]
    named = [rows[:, k : k + 1] == expert for k in range(top)]
    total = sum([m.astype(jnp.float32) for m in named])
    before = lax.broadcasted_iota(jnp.int32, (own_rows, own_rows), 1) < lax.broadcasted_iota(
        jnp.int32, (own_rows, own_rows), 0
    )
    rank = jnp.dot(
        before.astype(jnp.bfloat16), total.astype(jnp.bfloat16), preferred_element_type=jnp.float32
    )
    hit = rank == slot
    chosen = jnp.where(hit, total, 0.0)
    for k in range(top):
        mine = jnp.where(hit & named[k], 1.0, 0.0)
        sel[2 * k * own_rows : (2 * k + 1) * own_rows, :] = jnp.where(right, 0.0, mine).astype(
            jnp.bfloat16
        )
        sel[(2 * k + 1) * own_rows : (2 * k + 2) * own_rows, :] = jnp.where(
            right, mine, 0.0
        ).astype(jnp.bfloat16)
    spread = jnp.concatenate(
        [jnp.where(right, 0.0, chosen), jnp.where(right, chosen, 0.0)], axis=0
    )
    spread = spread.T.astype(jnp.bfloat16)
    load_x.wait()
    x = xbuf[...].astype(jnp.float32)
    scale = lax.rsqrt(jnp.mean(x * x, axis=-1, keepdims=True) + 1e-06)
    normed = (x * scale * gain_ref[...].astype(jnp.float32)).astype(jnp.bfloat16)
    stacked = jnp.concatenate([normed[:, :wide], normed[:, wide:]], axis=0)
    outgoing = jnp.dot(spread, stacked, preferred_element_type=jnp.float32)
    sbuf[...] = outgoing.astype(jnp.bfloat16).reshape(sbuf.shape)
    for s in range(1, n):
        send_a(s).start()
    keep = pltpu.make_async_copy(sbuf.at[e], recv.at[e, t], lsem.at[7])
    keep.start()
    keep.wait()
    copy_bx(0, t).start()
    copy_bc(0, t).start()

    for s in range(1, half):
        kv_far_in(s).wait_recv()
        kv_mate(s).start()
    for s in range(half):
        kv_mate_in(s).wait_recv()
    own_gate = gate_ref[:, pl.ds(pl.multiple_of(e * seq, seq), seq)]
    eye = lax.broadcasted_iota(jnp.int32, (seq, seq), 0) == lax.broadcasted_iota(
        jnp.int32, (seq, seq), 1
    )
    gate_col = jnp.sum(
        jnp.where(eye, jnp.broadcast_to(own_gate, (seq, seq)), 0.0), axis=1, keepdims=True
    )
    key_pos = lax.broadcasted_iota(jnp.int32, (seq, n * seq), 1)
    query_pos = lax.broadcasted_iota(jnp.int32, (seq, n * seq), 0) + e * seq
    bias = gate_col - gate_ref[...]
    group = q_ref.shape[1] // head
    heads_out = []
    for g in range(group):
        q = q_ref[:, g * head : (g + 1) * head]
        scores = jnp.concatenate(
            [
                jnp.dot(q, kv[j, 0:head, :], preferred_element_type=jnp.float32)
                for j in range(n)
            ],
            axis=1,
        )
        scores = scores * (head ** (-0.5)) + bias
        scores = jnp.where(key_pos <= query_pos, scores, -jnp.inf)
        weights = jnp.exp(scores - jnp.max(scores, axis=-1, keepdims=True))
        whole = jnp.sum(weights, axis=-1, keepdims=True)
        weights = weights.astype(jnp.bfloat16)
        summed = jnp.zeros((seq, head), jnp.float32)
        for j in range(n):
            summed = summed + lax.dot_general(
                weights[:, j * seq : (j + 1) * seq],
                kv[j, head : 2 * head, :],
                (((1,), (1,)), ((), ())),
                preferred_element_type=jnp.float32,
            )
        heads_out.append(summed / whole)
    attended = jnp.concatenate(heads_out, axis=1).astype(jnp.bfloat16)
    att[...] = attended.reshape(att.shape)
    attr[t] = att[t]

    def copy_att(s):
        dst = lax.rem(t + s, tpn)
        return remote(att.at[dst], attr.at[t], ats.at[s], atr.at[s], e, dst)

    def copy_att_in(s):
        src = lax.rem(t - s + tpn, tpn)
        return remote(att.at[src], attr.at[src], ats.at[s], atr.at[s], e, lax.rem(t + s, tpn))

    for s in range(1, tpn):
        copy_att(s).start()
    load_g.wait()
    load_u.wait()
    load_d.wait()

    def step(i, carry):
        @pl.when((i >= 1) & (i < n))
        def _():
            copy_a(i).wait_recv()
            copy_bx(i, t).start()
            copy_bc(i, t).start()

        @pl.when((i >= 1) & (i <= n))
        def _():
            copy_bx(i - 1, peer).wait_recv()
            copy_c(i - 1, peer).start()

        @pl.when((i >= 2) & (i <= n + 1))
        def _():
            s = i - 2
            src = source(s)
            copy_bc(s, partner).wait_recv()
            copy_c(s, opp).wait_recv()
            block = recv[src].astype(jnp.float32)
            count = block.shape[0] * cap
            lo = block[:, :cap].reshape(count, wide).astype(jnp.bfloat16)
            hi = block[:, cap:].reshape(count, wide).astype(jnp.bfloat16)
            gate = jnp.dot(lo, wgv[0:wide, :], preferred_element_type=jnp.float32) + jnp.dot(
                hi, wgv[wide:, :], preferred_element_type=jnp.float32
            )
            upper = jnp.dot(lo, wuv[0:wide, :], preferred_element_type=jnp.float32) + jnp.dot(
                hi, wuv[wide:, :], preferred_element_type=jnp.float32
            )
            hidden = (gate / (1.0 + jnp.exp(-gate)) * upper).astype(jnp.bfloat16)
            down = jnp.dot(hidden, wdv[...], preferred_element_type=jnp.float32)
            shape = (tpn, cap, wide)
            part[src] = jnp.concatenate(
                [down[:, :wide].reshape(shape), down[:, wide:].reshape(shape)], axis=1
            ).astype(jnp.bfloat16)
            copy_r1(s, 1, opp).start()
            copy_r1(s, 0, partner).start()

        @pl.when((i >= 3) & (i <= n + 2))
        def _():
            s = i - 3
            src = source(s)
            copy_r1(s, 1, opp).wait_recv()
            copy_r1(s, 0, partner).wait_recv()
            s2[src] = (
                part[src, peer].astype(jnp.float32) + r1[src, 1].astype(jnp.float32)
            ).astype(jnp.bfloat16)
            copy_r2(s).start()

        @pl.when(i >= 4)
        def _():
            s = i - 4
            src = source(s)
            copy_r2(s).wait_recv()
            s3[src] = (
                part[src, t].astype(jnp.float32)
                + r1[src, 0].astype(jnp.float32)
                + r2[src].astype(jnp.float32)
            ).astype(jnp.bfloat16)

            @pl.when(s > 0)
            def _():
                copy_r3(s).start()

            @pl.when(s == 0)
            def _():
                rbuf[e] = s3[e]

        return carry

    lax.fori_loop(1, n + 4, step, 0)

    for s in range(1, tpn):
        copy_att_in(s).wait_recv()
    load_o.wait()
    joined = jnp.concatenate([attr[j] for j in range(tpn)], axis=1)
    mixed_ref[...] = jnp.dot(joined, owv[...], preferred_element_type=jnp.float32).astype(
        jnp.bfloat16
    )

    for s in range(1, n):
        copy_r3_in(s).wait_recv()
    picked = jnp.dot(
        sel[...], rbuf[...].reshape(lanes, wide), preferred_element_type=jnp.float32
    )
    rw = rw_ref[pl.ds(pl.multiple_of(t * own_rows, own_rows), own_rows), :]
    for h in range(2):
        acc = jnp.zeros((own_rows, wide), jnp.float32)
        for k in range(top):
            at = (2 * k + h) * own_rows
            acc = acc + rw[:, k : k + 1] * picked[at : at + own_rows]
        out_ref[:, h * wide : (h + 1) * wide] = acc.astype(jnp.bfloat16)

    for s in range(1, half):
        kv_far(s).wait_send()
    for s in range(half):
        kv_mate(s).wait_send()
    for s in range(1, tpn):
        copy_att(s).wait_send()

    def drain(s, carry):
        copy_bx(s, t).wait_send()
        copy_bc(s, t).wait_send()
        copy_c(s, peer).wait_send()
        copy_r1(s, 0, partner).wait_send()
        copy_r1(s, 1, opp).wait_send()
        copy_r2(s).wait_send()

        @pl.when(s > 0)
        def _():
            send_a(s).wait_send()
            copy_r3(s).wait_send()

        return carry

    lax.fori_loop(0, n, drain, 0)


def fused_body(
    n,
    tpn,
    queries,
    key_cache,
    value_cache,
    cum_gate,
    out_weight,
    routed_input,
    norm_gain,
    routes,
    route_weight,
    expert_gate,
    expert_up,
    expert_down,
):
    seq = queries.shape[0]
    head = key_cache.shape[1]
    width = routed_input.shape[1]
    wide = width // 2
    own_rows = routed_input.shape[0] // tpn
    top = routes.shape[1]
    units = expert_gate.shape[2]
    cap = block_capacity(own_rows, top, n * expert_gate.shape[0])
    bf16 = jnp.bfloat16
    chunk = (2 * cap, wide)
    vmem = pl.BlockSpec(memory_space=pltpu.VMEM)
    anywhere = pl.BlockSpec(memory_space=pl.ANY)
    dma = pltpu.SemaphoreType.DMA
    mixed, out = pl.pallas_call(
        functools.partial(fused_kernel, n, tpn, cap),
        out_shape=(
            jax.ShapeDtypeStruct((seq // tpn, width), bf16),
            jax.ShapeDtypeStruct((own_rows, width), bf16),
        ),
        in_specs=[vmem] * 5 + [anywhere] * 7,
        out_specs=(vmem, vmem),
        scratch_shapes=[
            pltpu.VMEM((own_rows, width), bf16),
            pltpu.VMEM((width, units), bf16),
            pltpu.VMEM((width, units), bf16),
            pltpu.VMEM((units, width), bf16),
            pltpu.VMEM(out_weight.shape, bf16),
            pltpu.VMEM((n, 2 * head, seq), bf16),
            pltpu.VMEM((tpn, seq // tpn, queries.shape[1]), bf16),
            pltpu.VMEM((tpn, seq // tpn, queries.shape[1]), bf16),
            pltpu.VMEM((2 * top * own_rows, 2 * n * cap), bf16),
            pltpu.VMEM((n,) + chunk, bf16),
            pltpu.VMEM((n, tpn) + chunk, bf16),
            pltpu.VMEM((n, tpn) + chunk, bf16),
            pltpu.VMEM((n, 2) + chunk, bf16),
            pltpu.VMEM((n,) + chunk, bf16),
            pltpu.VMEM((n,) + chunk, bf16),
            pltpu.VMEM((n,) + chunk, bf16),
            pltpu.VMEM((n,) + chunk, bf16),
            dma((8,)),
            dma((n,)),
            dma((n,)),
            dma((tpn,)),
            dma((tpn,)),
        ]
        + [dma((n,))] * 8
        + [dma((n, 2))] * 2
        + [dma((n,))] * 4,
        compiler_params=pltpu.CompilerParams(
            collective_id=0, has_side_effects=True, vmem_limit_bytes=48 * 1024 * 1024
        ),
    )(
        queries,
        cum_gate,
        norm_gain.reshape(1, width),
        routes,
        route_weight,
        key_cache,
        value_cache,
        out_weight,
        routed_input,
        expert_gate,
        expert_up,
        expert_down,
    )
    return mixed, out


def block_capacity(own_rows, top_count, expert_count):
    return max(2, own_rows * top_count * 3 // (2 * expert_count))


def slot_chooser(route_rows, expert_count, capacity):
    token_rows, top_count = route_rows.shape
    flat = route_rows.reshape(token_rows * top_count)
    same = (flat[:, None] == jnp.arange(expert_count, dtype=jnp.int32)[None, :]).astype(jnp.int32)
    earlier = jnp.cumsum(same, axis=0) - same
    rank = jnp.sum(earlier * same, axis=1)
    slot = flat * capacity + rank
    chosen = slot[:, None] == jnp.arange(expert_count * capacity, dtype=jnp.int32)[None, :]
    return chosen.astype(jnp.bfloat16).reshape(token_rows, top_count, expert_count * capacity)


def rms_rows(source, norm_gain):
    widened = source.astype(jnp.float32)
    scale = lax.rsqrt(jnp.mean(widened * widened, axis=-1, keepdims=True) + 1e-06)
    return (widened * scale * norm_gain.astype(jnp.float32)).astype(jnp.bfloat16)


def mixer_half(queries, key_cache, value_cache, cum_gate, out_weight):
    seq_rows = queries.shape[0]
    local_heads = key_cache.shape[0]
    head_size = key_cache.shape[1]
    group = queries.shape[1] // (local_heads * head_size)
    own_start = lax.axis_index("ep") * seq_rows
    query_heads = queries.reshape(seq_rows, local_heads, group, head_size)
    query_pos = own_start + jnp.arange(seq_rows, dtype=jnp.int32)
    gate_query = lax.dynamic_slice_in_dim(cum_gate, own_start, seq_rows, 1)
    gate_rows = jnp.transpose(gate_query)[:, :, None, None]
    scale = head_size ** (-0.5)
    best_start = jnp.full((seq_rows, local_heads, group), -jnp.inf, jnp.float32)
    total_start = jnp.zeros((seq_rows, local_heads, group), jnp.float32)
    summed_start = jnp.zeros((seq_rows, local_heads * group * head_size), jnp.float32)
    pieces = (
        lax.all_gather(key_cache, "ep", axis=2, tiled=True),
        lax.all_gather(value_cache, "ep", axis=2, tiled=True),
    )

    def update(state):
        best, total, summed = state
        key_piece, value_piece = pieces
        width = key_piece.shape[2]
        scores = (
            jnp.einsum("thgd,hds->thgs", query_heads, key_piece, preferred_element_type=jnp.float32)
            * scale
        )
        scores = scores + gate_rows - cum_gate[None, :, None, :]
        key_pos = jnp.arange(width, dtype=jnp.int32)
        allowed = key_pos[None, :] <= query_pos[:, None]
        scores = jnp.where(allowed[:, None, None, :], scores, -jnp.inf)
        new_best = jnp.max(scores, axis=-1)
        factor = jnp.exp(best - new_best)
        weights = jnp.exp(scores - new_best[..., None])
        new_total = total * factor + jnp.sum(weights, axis=-1)
        product = jnp.einsum(
            "thgs,hds->thgd",
            weights.astype(jnp.bfloat16),
            value_piece,
            preferred_element_type=jnp.float32,
        )
        new_summed = summed.reshape(product.shape) * factor[..., None] + product
        return (new_best, new_total, new_summed.reshape(seq_rows, local_heads * group * head_size))

    best, total, summed = lax.cond(
        jnp.int32(0) <= own_start,
        update,
        lambda state: state,
        (best_start, total_start, summed_start),
    )
    attended = summed.reshape(seq_rows, local_heads, group, head_size) / total[..., None]
    attended = attended.astype(jnp.bfloat16).reshape(seq_rows, local_heads * group * head_size)
    by_position = lax.all_to_all(attended, "tp", split_axis=0, concat_axis=1, tiled=True)
    return jnp.dot(by_position, out_weight, preferred_element_type=jnp.float32).astype(jnp.bfloat16)


def expert_half(routed_input, norm_gain, routes, route_weight, expert_gate, expert_up, expert_down):
    group_size = lax.axis_size("tp")
    ep_size = lax.axis_size("ep")
    tp_index = lax.axis_index("tp")
    seq_rows, width = routed_input.shape
    own_rows = seq_rows // group_size
    local_experts = expert_gate.shape[0]
    expert_count = local_experts * ep_size
    top_count = routes.shape[1]
    capacity = max(2, own_rows * top_count * 3 // (2 * expert_count))
    per_device = local_experts * capacity
    mine = lax.dynamic_slice_in_dim(routed_input, tp_index * own_rows, own_rows, 0)
    own_routes = lax.dynamic_slice_in_dim(routes, tp_index * own_rows, own_rows, 0)
    chooser = slot_chooser(own_routes, expert_count, capacity)
    normed = rms_rows(mine, norm_gain)
    outgoing = jnp.einsum("tks,td->sd", chooser, normed, preferred_element_type=jnp.float32).astype(
        jnp.bfloat16
    )
    arrived = lax.all_to_all(
        outgoing.reshape(1, ep_size, per_device, width),
        "ep",
        split_axis=1,
        concat_axis=1,
        tiled=True,
    )
    received = lax.all_gather(arrived, "tp", axis=0, tiled=True)
    blocks = received.shape[0]
    divide_point = received.reshape(blocks, ep_size, local_experts, capacity, width)
    gate = jnp.einsum(
        "abecd,edf->abecf", divide_point, expert_gate, preferred_element_type=jnp.float32
    )
    upper = jnp.einsum(
        "abecd,edf->abecf", divide_point, expert_up, preferred_element_type=jnp.float32
    )
    hidden = (jax.nn.silu(gate) * upper).astype(jnp.bfloat16)
    partial_value = jnp.einsum(
        "abecf,efd->abecd", hidden, expert_down, preferred_element_type=jnp.float32
    )
    rounded = lax.optimization_barrier(partial_value.astype(jnp.bfloat16)).astype(jnp.float32)
    summed = lax.psum_scatter(
        rounded.reshape(lax.axis_size("tp") * 1, ep_size, per_device, width).astype(jnp.bfloat16),
        "tp",
        scatter_dimension=0,
        tiled=True,
    )
    returned = lax.all_to_all(summed, "ep", split_axis=1, concat_axis=1, tiled=True)
    picked = jnp.einsum(
        "tks,sd->tkd",
        chooser,
        returned.reshape(ep_size * per_device, width),
        preferred_element_type=jnp.float32,
    )
    own_weight = lax.dynamic_slice_in_dim(route_weight, tp_index * own_rows, own_rows, 0)
    return jnp.sum(own_weight[:, :, None] * picked, axis=1).astype(jnp.bfloat16)


def body(
    queries,
    key_cache,
    value_cache,
    cum_gate,
    out_weight,
    routed_input,
    norm_gain,
    routes,
    route_weight,
    expert_gate,
    expert_up,
    expert_down,
):
    mixed_out = mixer_half(queries, key_cache, value_cache, cum_gate, out_weight)
    expert_out = expert_half(
        routed_input, norm_gain, routes, route_weight, expert_gate, expert_up, expert_down
    )
    return (mixed_out, expert_out)


def pick_body(
    n,
    tpn,
    queries,
    key_cache,
    value_cache,
    cum_gate,
    out_weight,
    routed_input,
    norm_gain,
    routes,
    route_weight,
    expert_gate,
    *rest,
):
    seq, columns = queries.shape
    own_rows = routed_input.shape[0] // tpn
    cap = block_capacity(own_rows, routes.shape[1], n * expert_gate.shape[0])
    fits = (
        tpn == 4
        and n % 2 == 0
        and cap % 8 == 0
        and expert_gate.shape[0] == 1
        and key_cache.shape[0] == 1
        and seq % 128 == 0
    )
    args = (
        queries,
        key_cache,
        value_cache,
        cum_gate,
        out_weight,
        routed_input,
        norm_gain,
        routes,
        route_weight,
        expert_gate,
    ) + rest
    return fused_body(n, tpn, *args) if fits else body(*args)


def solution(mesh):
    return jax.shard_map(
        functools.partial(pick_body, mesh.shape["ep"], mesh.shape["tp"]),
        mesh=mesh,
        in_specs=(
            P("ep", "tp"),
            P("tp", None, "ep"),
            P("tp", None, "ep"),
            P("tp", None),
            P(),
            P("ep", None),
            P(),
            P("ep", None),
            P("ep", None),
            P("ep", None, "tp"),
            P("ep", None, "tp"),
            P("ep", "tp", None),
        ),
        out_specs=(P(("ep", "tp"), None), P(("ep", "tp"), None)),
        check_vma=False,
    )
```

```python
import functools

import jax
import jax.numpy as jnp
from jax import lax
from jax.experimental import pallas as pl
from jax.experimental.pallas import tpu as pltpu
from jax.sharding import PartitionSpec as P

MESH = pl.DeviceIdType.MESH


def fused_kernel(
    n,
    tpn,
    cap,
    q_any,
    gate_any,
    gain_any,
    routes_any,
    rw_any,
    k_any,
    v_any,
    ow_any,
    x_any,
    wg_any,
    wu_any,
    wd_any,
    mixed_ref,
    out_ref,
    q_ref,
    gate_ref,
    gain_ref,
    routes_ref,
    rw_ref,
    xbuf,
    wgv,
    wuv,
    wdv,
    owv,
    kv,
    att,
    attr,
    sel,
    sbuf,
    recv,
    part,
    r1,
    s2,
    r2,
    s3,
    rbuf,
    lsem,
    kvs,
    kvr,
    ats,
    atr,
    a_s,
    a_r,
    bx_s,
    bx_r,
    bc_s,
    bc_r,
    c_s,
    c_r,
    r1_s,
    r1_r,
    r2_s,
    r2_r,
    r3_s,
    r3_r,
):
    e = lax.axis_index("ep")
    t = lax.axis_index("tp")
    partner = t + 1 - 2 * lax.rem(t, 2)
    peer = lax.rem(t + 2, tpn)
    opp = lax.rem(partner + 2, tpn)
    mate = e + 1 - 2 * lax.rem(e, 2)
    half = n // 2
    own_rows, width = xbuf.shape
    wide = width // 2
    head = k_any.shape[1]
    seq = q_ref.shape[0]

    barrier = pltpu.get_barrier_semaphore()
    for s in range(1, n):
        pl.semaphore_signal(
            barrier, inc=1, device_id={"ep": lax.rem(e + s, n), "tp": t}, device_id_type=MESH
        )
    for s in range(1, tpn):
        pl.semaphore_signal(
            barrier, inc=1, device_id={"ep": e, "tp": lax.rem(t + s, tpn)}, device_id_type=MESH
        )

    load_x = pltpu.make_async_copy(x_any.at[pl.ds(t * own_rows, own_rows)], xbuf, lsem.at[0])
    load_k = pltpu.make_async_copy(k_any.at[0], kv.at[e, pl.ds(0, head)], lsem.at[1])
    load_v = pltpu.make_async_copy(v_any.at[0], kv.at[e, pl.ds(head, head)], lsem.at[2])
    load_g = pltpu.make_async_copy(wg_any.at[0], wgv, lsem.at[3])
    load_u = pltpu.make_async_copy(wu_any.at[0], wuv, lsem.at[4])
    load_d = pltpu.make_async_copy(wd_any.at[0], wdv, lsem.at[5])
    load_o = pltpu.make_async_copy(ow_any, owv, lsem.at[6])
    load_q = pltpu.make_async_copy(q_any, q_ref, lsem.at[8])
    load_c = pltpu.make_async_copy(gate_any, gate_ref, lsem.at[9])
    load_n = pltpu.make_async_copy(gain_any, gain_ref, lsem.at[10])
    load_r = pltpu.make_async_copy(routes_any, routes_ref, lsem.at[11])
    load_w = pltpu.make_async_copy(rw_any, rw_ref, lsem.at[12])
    load_k.start()
    load_v.start()
    load_x.start()
    load_r.start()
    load_n.start()
    load_w.start()
    load_q.start()
    load_c.start()
    load_g.start()
    load_u.start()
    load_d.start()
    load_o.start()

    def remote(src, dst, ssem, rsem, ep, tp):
        return pltpu.make_async_remote_copy(
            src_ref=src,
            dst_ref=dst,
            send_sem=ssem,
            recv_sem=rsem,
            device_id={"ep": ep, "tp": tp},
            device_id_type=MESH,
        )

    def kv_far(s):
        return remote(kv.at[e], kv.at[e], kvs.at[s], kvr.at[s], lax.rem(e + 2 * s, n), t)

    def kv_far_in(s):
        src = lax.rem(e - 2 * s + n, n)
        return remote(kv.at[src], kv.at[src], kvs.at[s], kvr.at[s], lax.rem(e + 2 * s, n), t)

    def kv_mate(s):
        src = lax.rem(e - 2 * s + n, n)
        return remote(kv.at[src], kv.at[src], kvs.at[half + s], kvr.at[half + s], mate, t)

    def kv_mate_in(s):
        src = lax.rem(mate - 2 * s + n, n)
        return remote(kv.at[src], kv.at[src], kvs.at[half + s], kvr.at[half + s], mate, t)

    def source(s):
        return lax.rem(e - s + n, n)

    def send_a(s):
        dst = lax.rem(e + s, n)
        return remote(sbuf.at[dst], recv.at[e, t], a_s.at[s], a_r.at[s], dst, t)

    def copy_a(s):
        src = source(s)
        return remote(sbuf.at[src], recv.at[src, t], a_s.at[s], a_r.at[s], lax.rem(e + s, n), t)

    def copy_bx(s, col):
        src = source(s)
        return remote(recv.at[src, col], recv.at[src, col], bx_s.at[s], bx_r.at[s], e, peer)

    def copy_bc(s, col):
        src = source(s)
        return remote(recv.at[src, col], recv.at[src, col], bc_s.at[s], bc_r.at[s], e, partner)

    def copy_c(s, col):
        src = source(s)
        return remote(recv.at[src, col], recv.at[src, col], c_s.at[s], c_r.at[s], e, partner)

    def copy_r1(s, which, col):
        src = source(s)
        return remote(
            part.at[src, col], r1.at[src, which], r1_s.at[s, which], r1_r.at[s, which], e, partner
        )

    def copy_r2(s):
        src = source(s)
        return remote(s2.at[src], r2.at[src], r2_s.at[s], r2_r.at[s], e, peer)

    def copy_r3(s):
        src = source(s)
        return remote(s3.at[src], rbuf.at[e], r3_s.at[s], r3_r.at[s], src, t)

    def copy_r3_in(s):
        src = lax.rem(e + s, n)
        return remote(s3.at[src], rbuf.at[src], r3_s.at[s], r3_r.at[s], source(s), t)

    load_k.wait()
    load_v.wait()
    pl.semaphore_wait(barrier, n - 1 + tpn - 1)
    for s in range(1, half):
        kv_far(s).start()
    kv_mate(0).start()

    lanes = 2 * n * cap
    place = lax.broadcasted_iota(jnp.int32, (own_rows, lanes), 1).astype(jnp.float32) + 0.5
    expert = jnp.floor(place / (2.0 * cap))
    inside = place - 0.5 - expert * (2.0 * cap)
    right = inside >= cap
    slot = jnp.where(right, inside - cap, inside)
    top, share = routes_ref.shape
    own = lax.broadcasted_iota(jnp.int32, (own_rows, share), 1) == (
        lax.broadcasted_iota(jnp.int32, (own_rows, share), 0) + t * own_rows
    )

    def column(line):
        return jnp.sum(
            jnp.where(own, jnp.broadcast_to(line, own.shape), 0.0), axis=1, keepdims=True
        )

    load_r.wait()
    named = [
        column(routes_ref[k : k + 1, :].astype(jnp.float32)) == expert for k in range(top)
    ]
    total = sum([m.astype(jnp.float32) for m in named])
    before = lax.broadcasted_iota(jnp.int32, (own_rows, own_rows), 1) < lax.broadcasted_iota(
        jnp.int32, (own_rows, own_rows), 0
    )
    rank = jnp.dot(
        before.astype(jnp.bfloat16), total.astype(jnp.bfloat16), preferred_element_type=jnp.float32
    )
    hit = rank == slot
    chosen = jnp.where(hit, total, 0.0)
    for k in range(top):
        mine = jnp.where(hit & named[k], 1.0, 0.0)
        sel[2 * k * own_rows : (2 * k + 1) * own_rows, :] = jnp.where(right, 0.0, mine).astype(
            jnp.bfloat16
        )
        sel[(2 * k + 1) * own_rows : (2 * k + 2) * own_rows, :] = jnp.where(
            right, mine, 0.0
        ).astype(jnp.bfloat16)
    spread = jnp.concatenate(
        [jnp.where(right, 0.0, chosen), jnp.where(right, chosen, 0.0)], axis=0
    )
    spread = spread.T.astype(jnp.bfloat16)
    load_x.wait()
    load_n.wait()
    x = xbuf[...].astype(jnp.float32)
    gain = gain_ref[...].astype(jnp.float32)
    gain = jnp.concatenate([gain[j : j + 1, :] for j in range(gain.shape[0])], axis=1)
    scale = lax.rsqrt(jnp.mean(x * x, axis=-1, keepdims=True) + 1e-06)
    normed = (x * scale * gain).astype(jnp.bfloat16)
    stacked = jnp.concatenate([normed[:, :wide], normed[:, wide:]], axis=0)
    outgoing = jnp.dot(spread, stacked, preferred_element_type=jnp.float32)
    sbuf[...] = outgoing.astype(jnp.bfloat16).reshape(sbuf.shape)
    for s in range(1, n):
        send_a(s).start()
    keep = pltpu.make_async_copy(sbuf.at[e], recv.at[e, t], lsem.at[7])
    keep.start()
    keep.wait()
    copy_bx(0, t).start()
    copy_bc(0, t).start()

    for s in range(1, half):
        kv_far_in(s).wait_recv()
        kv_mate(s).start()
    for s in range(half):
        kv_mate_in(s).wait_recv()
    load_q.wait()
    load_c.wait()
    own_gate = gate_ref[:, pl.ds(pl.multiple_of(e * seq, seq), seq)]
    eye = lax.broadcasted_iota(jnp.int32, (seq, seq), 0) == lax.broadcasted_iota(
        jnp.int32, (seq, seq), 1
    )
    gate_col = jnp.sum(
        jnp.where(eye, jnp.broadcast_to(own_gate, (seq, seq)), 0.0), axis=1, keepdims=True
    )
    key_pos = lax.broadcasted_iota(jnp.int32, (seq, n * seq), 1)
    query_pos = lax.broadcasted_iota(jnp.int32, (seq, n * seq), 0) + e * seq
    bias = gate_col - gate_ref[...]
    group = q_ref.shape[1] // head
    heads_out = []
    for g in range(group):
        q = q_ref[:, g * head : (g + 1) * head]
        scores = jnp.concatenate(
            [
                jnp.dot(q, kv[j, 0:head, :], preferred_element_type=jnp.float32)
                for j in range(n)
            ],
            axis=1,
        )
        scores = scores * (head ** (-0.5)) + bias
        scores = jnp.where(key_pos <= query_pos, scores, -jnp.inf)
        weights = jnp.exp(scores - jnp.max(scores, axis=-1, keepdims=True))
        whole = jnp.sum(weights, axis=-1, keepdims=True)
        weights = weights.astype(jnp.bfloat16)
        summed = jnp.zeros((seq, head), jnp.float32)
        for j in range(n):
            summed = summed + lax.dot_general(
                weights[:, j * seq : (j + 1) * seq],
                kv[j, head : 2 * head, :],
                (((1,), (1,)), ((), ())),
                preferred_element_type=jnp.float32,
            )
        heads_out.append(summed / whole)
    attended = jnp.concatenate(heads_out, axis=1).astype(jnp.bfloat16)
    att[...] = attended.reshape(att.shape)
    attr[t] = att[t]

    def copy_att(s):
        dst = lax.rem(t + s, tpn)
        return remote(att.at[dst], attr.at[t], ats.at[s], atr.at[s], e, dst)

    def copy_att_in(s):
        src = lax.rem(t - s + tpn, tpn)
        return remote(att.at[src], attr.at[src], ats.at[s], atr.at[s], e, lax.rem(t + s, tpn))

    for s in range(1, tpn):
        copy_att(s).start()
    load_g.wait()
    load_u.wait()
    load_d.wait()

    def step(i, carry):
        @pl.when((i >= 1) & (i < n))
        def _():
            copy_a(i).wait_recv()
            copy_bx(i, t).start()
            copy_bc(i, t).start()

        @pl.when((i >= 1) & (i <= n))
        def _():
            copy_bx(i - 1, peer).wait_recv()
            copy_c(i - 1, peer).start()

        @pl.when((i >= 2) & (i <= n + 1))
        def _():
            s = i - 2
            src = source(s)
            copy_bc(s, partner).wait_recv()
            copy_c(s, opp).wait_recv()
            block = recv[src].astype(jnp.float32)
            count = block.shape[0] * cap
            lo = block[:, :cap].reshape(count, wide).astype(jnp.bfloat16)
            hi = block[:, cap:].reshape(count, wide).astype(jnp.bfloat16)
            gate = jnp.dot(lo, wgv[0:wide, :], preferred_element_type=jnp.float32) + jnp.dot(
                hi, wgv[wide:, :], preferred_element_type=jnp.float32
            )
            upper = jnp.dot(lo, wuv[0:wide, :], preferred_element_type=jnp.float32) + jnp.dot(
                hi, wuv[wide:, :], preferred_element_type=jnp.float32
            )
            hidden = (gate / (1.0 + jnp.exp(-gate)) * upper).astype(jnp.bfloat16)
            down = jnp.dot(hidden, wdv[...], preferred_element_type=jnp.float32)
            shape = (tpn, cap, wide)
            part[src] = jnp.concatenate(
                [down[:, :wide].reshape(shape), down[:, wide:].reshape(shape)], axis=1
            ).astype(jnp.bfloat16)
            copy_r1(s, 1, opp).start()
            copy_r1(s, 0, partner).start()

        @pl.when((i >= 3) & (i <= n + 2))
        def _():
            s = i - 3
            src = source(s)
            copy_r1(s, 1, opp).wait_recv()
            copy_r1(s, 0, partner).wait_recv()
            s2[src] = (
                part[src, peer].astype(jnp.float32) + r1[src, 1].astype(jnp.float32)
            ).astype(jnp.bfloat16)
            copy_r2(s).start()

        @pl.when(i >= 4)
        def _():
            s = i - 4
            src = source(s)
            copy_r2(s).wait_recv()
            s3[src] = (
                part[src, t].astype(jnp.float32)
                + r1[src, 0].astype(jnp.float32)
                + r2[src].astype(jnp.float32)
            ).astype(jnp.bfloat16)

            @pl.when(s > 0)
            def _():
                copy_r3(s).start()

            @pl.when(s == 0)
            def _():
                rbuf[e] = s3[e]

        return carry

    lax.fori_loop(1, n + 4, step, 0)

    for s in range(1, tpn):
        copy_att_in(s).wait_recv()
    load_o.wait()
    joined = jnp.concatenate([attr[j] for j in range(tpn)], axis=1)
    mixed_ref[...] = jnp.dot(joined, owv[...], preferred_element_type=jnp.float32).astype(
        jnp.bfloat16
    )

    for s in range(1, n):
        copy_r3_in(s).wait_recv()
    picked = jnp.dot(
        sel[...], rbuf[...].reshape(lanes, wide), preferred_element_type=jnp.float32
    )
    load_w.wait()
    rw = [column(rw_ref[k : k + 1, :]) for k in range(top)]
    for h in range(2):
        acc = jnp.zeros((own_rows, wide), jnp.float32)
        for k in range(top):
            at = (2 * k + h) * own_rows
            acc = acc + rw[k] * picked[at : at + own_rows]
        out_ref[:, h * wide : (h + 1) * wide] = acc.astype(jnp.bfloat16)

    for s in range(1, half):
        kv_far(s).wait_send()
    for s in range(half):
        kv_mate(s).wait_send()
    for s in range(1, tpn):
        copy_att(s).wait_send()

    def drain(s, carry):
        copy_bx(s, t).wait_send()
        copy_bc(s, t).wait_send()
        copy_c(s, peer).wait_send()
        copy_r1(s, 0, partner).wait_send()
        copy_r1(s, 1, opp).wait_send()
        copy_r2(s).wait_send()

        @pl.when(s > 0)
        def _():
            send_a(s).wait_send()
            copy_r3(s).wait_send()

        return carry

    lax.fori_loop(0, n, drain, 0)


def fused_body(
    n,
    tpn,
    queries,
    key_cache,
    value_cache,
    cum_gate,
    out_weight,
    routed_input,
    norm_gain,
    routes,
    route_weight,
    expert_gate,
    expert_up,
    expert_down,
):
    seq = queries.shape[0]
    head = key_cache.shape[1]
    width = routed_input.shape[1]
    wide = width // 2
    own_rows = routed_input.shape[0] // tpn
    top = routes.shape[1]
    units = expert_gate.shape[2]
    cap = block_capacity(own_rows, top, n * expert_gate.shape[0])
    bf16 = jnp.bfloat16
    chunk = (2 * cap, wide)
    vmem = pl.BlockSpec(memory_space=pltpu.VMEM)
    anywhere = pl.BlockSpec(memory_space=pltpu.HBM)
    dma = pltpu.SemaphoreType.DMA
    mixed, out = pl.pallas_call(
        functools.partial(fused_kernel, n, tpn, cap),
        out_shape=(
            jax.ShapeDtypeStruct((seq // tpn, width), bf16),
            jax.ShapeDtypeStruct((own_rows, width), bf16),
        ),
        in_specs=[anywhere] * 12,
        out_specs=(vmem, vmem),
        scratch_shapes=[
            pltpu.VMEM(queries.shape, bf16),
            pltpu.VMEM(cum_gate.shape, jnp.float32),
            pltpu.VMEM((width // 128, 128), bf16),
            pltpu.VMEM((top, tpn * own_rows), jnp.int32),
            pltpu.VMEM((top, tpn * own_rows), jnp.float32),
            pltpu.VMEM((own_rows, width), bf16),
            pltpu.VMEM((width, units), bf16),
            pltpu.VMEM((width, units), bf16),
            pltpu.VMEM((units, width), bf16),
            pltpu.VMEM(out_weight.shape, bf16),
            pltpu.VMEM((n, 2 * head, seq), bf16),
            pltpu.VMEM((tpn, seq // tpn, queries.shape[1]), bf16),
            pltpu.VMEM((tpn, seq // tpn, queries.shape[1]), bf16),
            pltpu.VMEM((2 * top * own_rows, 2 * n * cap), bf16),
            pltpu.VMEM((n,) + chunk, bf16),
            pltpu.VMEM((n, tpn) + chunk, bf16),
            pltpu.VMEM((n, tpn) + chunk, bf16),
            pltpu.VMEM((n, 2) + chunk, bf16),
            pltpu.VMEM((n,) + chunk, bf16),
            pltpu.VMEM((n,) + chunk, bf16),
            pltpu.VMEM((n,) + chunk, bf16),
            pltpu.VMEM((n,) + chunk, bf16),
            dma((13,)),
            dma((n,)),
            dma((n,)),
            dma((tpn,)),
            dma((tpn,)),
        ]
        + [dma((n,))] * 8
        + [dma((n, 2))] * 2
        + [dma((n,))] * 4,
        compiler_params=pltpu.CompilerParams(
            collective_id=0, has_side_effects=True, vmem_limit_bytes=60 * 1024 * 1024
        ),
    )(
        queries,
        cum_gate,
        norm_gain.reshape(width // 128, 128),
        routes.T,
        route_weight.T,
        key_cache,
        value_cache,
        out_weight,
        routed_input,
        expert_gate,
        expert_up,
        expert_down,
    )
    return mixed, out


def block_capacity(own_rows, top_count, expert_count):
    return max(2, own_rows * top_count * 3 // (2 * expert_count))


def slot_chooser(route_rows, expert_count, capacity):
    token_rows, top_count = route_rows.shape
    flat = route_rows.reshape(token_rows * top_count)
    same = (flat[:, None] == jnp.arange(expert_count, dtype=jnp.int32)[None, :]).astype(jnp.int32)
    earlier = jnp.cumsum(same, axis=0) - same
    rank = jnp.sum(earlier * same, axis=1)
    slot = flat * capacity + rank
    chosen = slot[:, None] == jnp.arange(expert_count * capacity, dtype=jnp.int32)[None, :]
    return chosen.astype(jnp.bfloat16).reshape(token_rows, top_count, expert_count * capacity)


def rms_rows(source, norm_gain):
    widened = source.astype(jnp.float32)
    scale = lax.rsqrt(jnp.mean(widened * widened, axis=-1, keepdims=True) + 1e-06)
    return (widened * scale * norm_gain.astype(jnp.float32)).astype(jnp.bfloat16)


def mixer_half(queries, key_cache, value_cache, cum_gate, out_weight):
    seq_rows = queries.shape[0]
    local_heads = key_cache.shape[0]
    head_size = key_cache.shape[1]
    group = queries.shape[1] // (local_heads * head_size)
    own_start = lax.axis_index("ep") * seq_rows
    query_heads = queries.reshape(seq_rows, local_heads, group, head_size)
    query_pos = own_start + jnp.arange(seq_rows, dtype=jnp.int32)
    gate_query = lax.dynamic_slice_in_dim(cum_gate, own_start, seq_rows, 1)
    gate_rows = jnp.transpose(gate_query)[:, :, None, None]
    scale = head_size ** (-0.5)
    best_start = jnp.full((seq_rows, local_heads, group), -jnp.inf, jnp.float32)
    total_start = jnp.zeros((seq_rows, local_heads, group), jnp.float32)
    summed_start = jnp.zeros((seq_rows, local_heads * group * head_size), jnp.float32)
    pieces = (
        lax.all_gather(key_cache, "ep", axis=2, tiled=True),
        lax.all_gather(value_cache, "ep", axis=2, tiled=True),
    )

    def update(state):
        best, total, summed = state
        key_piece, value_piece = pieces
        width = key_piece.shape[2]
        scores = (
            jnp.einsum("thgd,hds->thgs", query_heads, key_piece, preferred_element_type=jnp.float32)
            * scale
        )
        scores = scores + gate_rows - cum_gate[None, :, None, :]
        key_pos = jnp.arange(width, dtype=jnp.int32)
        allowed = key_pos[None, :] <= query_pos[:, None]
        scores = jnp.where(allowed[:, None, None, :], scores, -jnp.inf)
        new_best = jnp.max(scores, axis=-1)
        factor = jnp.exp(best - new_best)
        weights = jnp.exp(scores - new_best[..., None])
        new_total = total * factor + jnp.sum(weights, axis=-1)
        product = jnp.einsum(
            "thgs,hds->thgd",
            weights.astype(jnp.bfloat16),
            value_piece,
            preferred_element_type=jnp.float32,
        )
        new_summed = summed.reshape(product.shape) * factor[..., None] + product
        return (new_best, new_total, new_summed.reshape(seq_rows, local_heads * group * head_size))

    best, total, summed = lax.cond(
        jnp.int32(0) <= own_start,
        update,
        lambda state: state,
        (best_start, total_start, summed_start),
    )
    attended = summed.reshape(seq_rows, local_heads, group, head_size) / total[..., None]
    attended = attended.astype(jnp.bfloat16).reshape(seq_rows, local_heads * group * head_size)
    by_position = lax.all_to_all(attended, "tp", split_axis=0, concat_axis=1, tiled=True)
    return jnp.dot(by_position, out_weight, preferred_element_type=jnp.float32).astype(jnp.bfloat16)


def expert_half(routed_input, norm_gain, routes, route_weight, expert_gate, expert_up, expert_down):
    group_size = lax.axis_size("tp")
    ep_size = lax.axis_size("ep")
    tp_index = lax.axis_index("tp")
    seq_rows, width = routed_input.shape
    own_rows = seq_rows // group_size
    local_experts = expert_gate.shape[0]
    expert_count = local_experts * ep_size
    top_count = routes.shape[1]
    capacity = max(2, own_rows * top_count * 3 // (2 * expert_count))
    per_device = local_experts * capacity
    mine = lax.dynamic_slice_in_dim(routed_input, tp_index * own_rows, own_rows, 0)
    own_routes = lax.dynamic_slice_in_dim(routes, tp_index * own_rows, own_rows, 0)
    chooser = slot_chooser(own_routes, expert_count, capacity)
    normed = rms_rows(mine, norm_gain)
    outgoing = jnp.einsum("tks,td->sd", chooser, normed, preferred_element_type=jnp.float32).astype(
        jnp.bfloat16
    )
    arrived = lax.all_to_all(
        outgoing.reshape(1, ep_size, per_device, width),
        "ep",
        split_axis=1,
        concat_axis=1,
        tiled=True,
    )
    received = lax.all_gather(arrived, "tp", axis=0, tiled=True)
    blocks = received.shape[0]
    divide_point = received.reshape(blocks, ep_size, local_experts, capacity, width)
    gate = jnp.einsum(
        "abecd,edf->abecf", divide_point, expert_gate, preferred_element_type=jnp.float32
    )
    upper = jnp.einsum(
        "abecd,edf->abecf", divide_point, expert_up, preferred_element_type=jnp.float32
    )
    hidden = (jax.nn.silu(gate) * upper).astype(jnp.bfloat16)
    partial_value = jnp.einsum(
        "abecf,efd->abecd", hidden, expert_down, preferred_element_type=jnp.float32
    )
    rounded = lax.optimization_barrier(partial_value.astype(jnp.bfloat16)).astype(jnp.float32)
    summed = lax.psum_scatter(
        rounded.reshape(lax.axis_size("tp") * 1, ep_size, per_device, width).astype(jnp.bfloat16),
        "tp",
        scatter_dimension=0,
        tiled=True,
    )
    returned = lax.all_to_all(summed, "ep", split_axis=1, concat_axis=1, tiled=True)
    picked = jnp.einsum(
        "tks,sd->tkd",
        chooser,
        returned.reshape(ep_size * per_device, width),
        preferred_element_type=jnp.float32,
    )
    own_weight = lax.dynamic_slice_in_dim(route_weight, tp_index * own_rows, own_rows, 0)
    return jnp.sum(own_weight[:, :, None] * picked, axis=1).astype(jnp.bfloat16)


def body(
    queries,
    key_cache,
    value_cache,
    cum_gate,
    out_weight,
    routed_input,
    norm_gain,
    routes,
    route_weight,
    expert_gate,
    expert_up,
    expert_down,
):
    mixed_out = mixer_half(queries, key_cache, value_cache, cum_gate, out_weight)
    expert_out = expert_half(
        routed_input, norm_gain, routes, route_weight, expert_gate, expert_up, expert_down
    )
    return (mixed_out, expert_out)


def pick_body(
    n,
    tpn,
    queries,
    key_cache,
    value_cache,
    cum_gate,
    out_weight,
    routed_input,
    norm_gain,
    routes,
    route_weight,
    expert_gate,
    *rest,
):
    seq, columns = queries.shape
    own_rows = routed_input.shape[0] // tpn
    cap = block_capacity(own_rows, routes.shape[1], n * expert_gate.shape[0])
    fits = (
        tpn == 4
        and n % 2 == 0
        and cap % 8 == 0
        and expert_gate.shape[0] == 1
        and key_cache.shape[0] == 1
        and seq % 128 == 0
    )
    args = (
        queries,
        key_cache,
        value_cache,
        cum_gate,
        out_weight,
        routed_input,
        norm_gain,
        routes,
        route_weight,
        expert_gate,
    ) + rest
    return fused_body(n, tpn, *args) if fits else body(*args)


def solution(mesh):
    return jax.shard_map(
        functools.partial(pick_body, mesh.shape["ep"], mesh.shape["tp"]),
        mesh=mesh,
        in_specs=(
            P("ep", "tp"),
            P("tp", None, "ep"),
            P("tp", None, "ep"),
            P("tp", None),
            P(),
            P("ep", None),
            P(),
            P("ep", None),
            P("ep", None),
            P("ep", None, "tp"),
            P("ep", None, "tp"),
            P("ep", "tp", None),
        ),
        out_specs=(P(("ep", "tp"), None), P(("ep", "tp"), None)),
        check_vma=False,
    )
```

```python
import functools

import jax
import jax.numpy as jnp
from jax import lax
from jax.experimental import pallas as pl
from jax.experimental.pallas import tpu as pltpu
from jax.sharding import PartitionSpec as P

MESH = pl.DeviceIdType.MESH


def fused_kernel(
    n,
    tpn,
    cap,
    q_any,
    gate_any,
    gain_any,
    routes_any,
    rw_any,
    k_any,
    v_any,
    ow_any,
    x_any,
    wg_any,
    wu_any,
    wd_any,
    mixed_ref,
    out_ref,
    q_ref,
    gate_ref,
    gain_ref,
    routes_ref,
    rw_ref,
    xbuf,
    wgv,
    wuv,
    wdv,
    owv,
    kv,
    att,
    attr,
    sel,
    sbuf,
    sbuf2,
    recv,
    part,
    r1,
    s2,
    r2,
    s3,
    rbuf,
    lsem,
    kvs,
    kvr,
    ats,
    atr,
    a_s,
    a_r,
    bx_s,
    bx_r,
    bc_s,
    bc_r,
    c_s,
    c_r,
    r1_s,
    r1_r,
    r2_s,
    r2_r,
    r3_s,
    r3_r,
):
    e = lax.axis_index("ep")
    t = lax.axis_index("tp")
    partner = t + 1 - 2 * lax.rem(t, 2)
    peer = lax.rem(t + 2, tpn)
    opp = lax.rem(partner + 2, tpn)
    mate = e + 1 - 2 * lax.rem(e, 2)
    half = n // 2
    _, own_rows, width = xbuf.shape
    wide = width // 2
    head = k_any.shape[1]
    seq = q_ref.shape[0]

    barrier = pltpu.get_barrier_semaphore()
    for s in range(1, n):
        pl.semaphore_signal(
            barrier, inc=1, device_id={"ep": lax.rem(e + s, n), "tp": t}, device_id_type=MESH
        )
    for s in range(1, tpn):
        pl.semaphore_signal(
            barrier, inc=1, device_id={"ep": e, "tp": lax.rem(t + s, tpn)}, device_id_type=MESH
        )

    def load_x(j):
        at = lax.rem(t + j, tpn) * own_rows
        return pltpu.make_async_copy(x_any.at[pl.ds(at, own_rows)], xbuf.at[j], lsem.at[12 + j])

    load_k = pltpu.make_async_copy(k_any.at[0], kv.at[e, pl.ds(0, head)], lsem.at[1])
    load_v = pltpu.make_async_copy(v_any.at[0], kv.at[e, pl.ds(head, head)], lsem.at[2])
    load_g = pltpu.make_async_copy(wg_any.at[0], wgv, lsem.at[3])
    load_u = pltpu.make_async_copy(wu_any.at[0], wuv, lsem.at[4])
    load_d = pltpu.make_async_copy(wd_any.at[0], wdv, lsem.at[5])
    load_o = pltpu.make_async_copy(ow_any, owv, lsem.at[6])
    load_q = pltpu.make_async_copy(q_any, q_ref, lsem.at[8])
    load_c = pltpu.make_async_copy(gate_any, gate_ref, lsem.at[9])
    load_n = pltpu.make_async_copy(gain_any, gain_ref, lsem.at[10])
    load_r = pltpu.make_async_copy(routes_any, routes_ref, lsem.at[11])
    load_w = pltpu.make_async_copy(rw_any, rw_ref, lsem.at[0])
    load_k.start()
    load_v.start()
    load_x(0).start()
    load_r.start()
    load_n.start()
    load_w.start()
    load_q.start()
    load_c.start()
    for j in range(1, tpn):
        load_x(j).start()
    load_g.start()
    load_u.start()
    load_d.start()
    load_o.start()

    def remote(src, dst, ssem, rsem, ep, tp):
        return pltpu.make_async_remote_copy(
            src_ref=src,
            dst_ref=dst,
            send_sem=ssem,
            recv_sem=rsem,
            device_id={"ep": ep, "tp": tp},
            device_id_type=MESH,
        )

    def kv_far(s):
        return remote(kv.at[e], kv.at[e], kvs.at[s], kvr.at[s], lax.rem(e + 2 * s, n), t)

    def kv_far_in(s):
        src = lax.rem(e - 2 * s + n, n)
        return remote(kv.at[src], kv.at[src], kvs.at[s], kvr.at[s], lax.rem(e + 2 * s, n), t)

    def kv_mate(s):
        src = lax.rem(e - 2 * s + n, n)
        return remote(kv.at[src], kv.at[src], kvs.at[half + s], kvr.at[half + s], mate, t)

    def kv_mate_in(s):
        src = lax.rem(mate - 2 * s + n, n)
        return remote(kv.at[src], kv.at[src], kvs.at[half + s], kvr.at[half + s], mate, t)

    def source(s):
        s = jnp.int32(s)
        flipped = jnp.int32(0)
        bit = 1
        while bit < n:
            ours = lax.rem(lax.div(e, jnp.int32(bit)), jnp.int32(2))
            theirs = lax.rem(lax.div(s, jnp.int32(bit)), jnp.int32(2))
            flipped = flipped + bit * (ours + theirs - 2 * ours * theirs)
            bit *= 2
        return flipped

    def send_a(s):
        dst = source(s)
        return remote(sbuf.at[dst], recv.at[e, t], a_s.at[s], a_r.at[s], dst, t)

    def send_near(s):
        dst = source(s)
        return remote(sbuf2.at[dst], recv.at[e, peer], bx_s.at[s], bx_r.at[s], dst, t)

    def copy_a(s):
        src = source(s)
        return remote(sbuf.at[src], recv.at[src, t], a_s.at[s], a_r.at[s], src, t)

    def copy_bx(s, col):
        src = source(s)
        return remote(recv.at[src, col], recv.at[src, col], bx_s.at[s], bx_r.at[s], e, peer)

    def copy_bc(s, col):
        src = source(s)
        return remote(recv.at[src, col], recv.at[src, col], bc_s.at[s], bc_r.at[s], e, partner)

    def copy_c(s, col):
        src = source(s)
        return remote(recv.at[src, col], recv.at[src, col], c_s.at[s], c_r.at[s], e, partner)

    def copy_r1(s, which, col):
        src = source(s)
        return remote(
            part.at[src, col], r1.at[src, which], r1_s.at[s, which], r1_r.at[s, which], e, partner
        )

    def copy_r2(s):
        src = source(s)
        return remote(s2.at[src], r2.at[src], r2_s.at[s], r2_r.at[s], e, peer)

    def copy_r3(s):
        src = source(s)
        return remote(s3.at[src], rbuf.at[e], r3_s.at[s], r3_r.at[s], src, t)

    def copy_r3_in(s):
        src = source(s)
        return remote(s3.at[src], rbuf.at[src], r3_s.at[s], r3_r.at[s], src, t)

    pl.semaphore_wait(barrier, n - 1 + tpn - 1)

    lanes = 2 * n * cap
    place = lax.broadcasted_iota(jnp.int32, (own_rows, lanes), 1).astype(jnp.float32) + 0.5
    expert = jnp.floor(place / (2.0 * cap))
    inside = place - 0.5 - expert * (2.0 * cap)
    right = inside >= cap
    slot = jnp.where(right, inside - cap, inside)
    top, share = routes_ref.shape

    def column(line, j):
        at = lax.rem(t + j, tpn) * own_rows
        own = lax.broadcasted_iota(jnp.int32, (own_rows, share), 1) == (
            lax.broadcasted_iota(jnp.int32, (own_rows, share), 0) + at
        )
        return jnp.sum(
            jnp.where(own, jnp.broadcast_to(line, own.shape), 0.0), axis=1, keepdims=True
        )

    def route(k, j):
        return column(routes_ref[k : k + 1, :].astype(jnp.float32), j)

    before = lax.broadcasted_iota(jnp.int32, (own_rows, own_rows), 1) < lax.broadcasted_iota(
        jnp.int32, (own_rows, own_rows), 0
    )

    def choose(j):
        named = [route(k, j) == expert for k in range(top)]
        total = sum([m.astype(jnp.float32) for m in named])
        rank = jnp.dot(
            before.astype(jnp.bfloat16),
            total.astype(jnp.bfloat16),
            preferred_element_type=jnp.float32,
        )
        hit = rank == slot
        chosen = jnp.where(hit, total, 0.0)
        spread = jnp.concatenate(
            [jnp.where(right, 0.0, chosen), jnp.where(right, chosen, 0.0)], axis=0
        )
        return spread.T.astype(jnp.bfloat16), hit, named

    load_r.wait()
    spread, hit, named = choose(0)
    load_n.wait()
    gain = gain_ref[...].astype(jnp.float32)
    gain = jnp.concatenate([gain[j : j + 1, :] for j in range(gain.shape[0])], axis=1)

    def halves(j):
        load_x(j).wait()
        x = xbuf[j].astype(jnp.float32)
        scale = lax.rsqrt(jnp.mean(x * x, axis=-1, keepdims=True) + 1e-06)
        normed = (x * scale * gain).astype(jnp.bfloat16)
        return jnp.concatenate([normed[:, :wide], normed[:, wide:]], axis=0)

    stacked = halves(0)
    outgoing = jnp.dot(spread, stacked, preferred_element_type=jnp.float32)
    sbuf[...] = outgoing.astype(jnp.bfloat16).reshape(sbuf.shape)
    for s in range(half, n):
        send_a(s).start()
    for s in range(1, half):
        send_a(s).start()
    keep = pltpu.make_async_copy(sbuf.at[e], recv.at[e, t], lsem.at[7])
    keep.start()
    outgoing = jnp.dot(choose(2)[0], halves(2), preferred_element_type=jnp.float32)
    sbuf2[...] = outgoing.astype(jnp.bfloat16).reshape(sbuf2.shape)
    for s in range(1, half):
        send_near(s).start()
    recv[e, peer] = sbuf2[e]
    keep.wait()
    for k in range(top):
        mine = jnp.where(hit & named[k], 1.0, 0.0)
        sel[2 * k * own_rows : (2 * k + 1) * own_rows, :] = jnp.where(right, 0.0, mine).astype(
            jnp.bfloat16
        )
        sel[(2 * k + 1) * own_rows : (2 * k + 2) * own_rows, :] = jnp.where(
            right, mine, 0.0
        ).astype(jnp.bfloat16)
    load_k.wait()
    load_v.wait()
    for s in range(1, half):
        kv_far(s).start()
    kv_mate(0).start()

    lane = lax.broadcasted_iota(jnp.int32, (own_rows, 2 * cap), 1)
    lane_right = lane >= cap
    lane_slot = jnp.where(lane_right, lane - cap, lane).astype(jnp.float32)
    mine_expert = e.astype(jnp.float32)
    for j in (1, 3):
        hits = sum(
            [jnp.where(route(k, j) == mine_expert, 1.0, 0.0) for k in range(top)]
        )
        hits = jnp.broadcast_to(hits, lane.shape)
        ranks = jnp.dot(
            before.astype(jnp.bfloat16),
            hits.astype(jnp.bfloat16),
            preferred_element_type=jnp.float32,
        )
        here = jnp.where(ranks == lane_slot, hits, 0.0)
        here = jnp.concatenate(
            [jnp.where(lane_right, 0.0, here), jnp.where(lane_right, here, 0.0)], axis=0
        )
        recv[e, lax.rem(t + j, tpn)] = jnp.dot(
            here.T.astype(jnp.bfloat16), halves(j), preferred_element_type=jnp.float32
        ).astype(jnp.bfloat16)

    def copy_att(s):
        dst = lax.rem(t + s, tpn)
        return remote(att.at[dst], attr.at[t], ats.at[s], atr.at[s], e, dst)

    def copy_att_in(s):
        src = lax.rem(t - s + tpn, tpn)
        return remote(att.at[src], attr.at[src], ats.at[s], atr.at[s], e, lax.rem(t + s, tpn))

    def attention():
        for s in range(half):
            kv_mate_in(s).wait_recv()
        load_q.wait()
        load_c.wait()
        own_gate = gate_ref[:, pl.ds(pl.multiple_of(e * seq, seq), seq)]
        eye = lax.broadcasted_iota(jnp.int32, (seq, seq), 0) == lax.broadcasted_iota(
            jnp.int32, (seq, seq), 1
        )
        gate_col = jnp.sum(
            jnp.where(eye, jnp.broadcast_to(own_gate, (seq, seq)), 0.0), axis=1, keepdims=True
        )
        key_pos = lax.broadcasted_iota(jnp.int32, (seq, n * seq), 1)
        query_pos = lax.broadcasted_iota(jnp.int32, (seq, n * seq), 0) + e * seq
        bias = gate_col - gate_ref[...]
        group = q_ref.shape[1] // head
        heads_out = []
        for g in range(group):
            q = q_ref[:, g * head : (g + 1) * head]
            scores = jnp.concatenate(
                [
                    jnp.dot(q, kv[j, 0:head, :], preferred_element_type=jnp.float32)
                    for j in range(n)
                ],
                axis=1,
            )
            scores = scores * (head ** (-0.5)) + bias
            scores = jnp.where(key_pos <= query_pos, scores, -jnp.inf)
            weights = jnp.exp(scores - jnp.max(scores, axis=-1, keepdims=True))
            whole = jnp.sum(weights, axis=-1, keepdims=True)
            weights = weights.astype(jnp.bfloat16)
            summed = jnp.zeros((seq, head), jnp.float32)
            for j in range(n):
                summed = summed + lax.dot_general(
                    weights[:, j * seq : (j + 1) * seq],
                    kv[j, head : 2 * head, :],
                    (((1,), (1,)), ((), ())),
                    preferred_element_type=jnp.float32,
                )
            heads_out.append(summed / whole)
        attended = jnp.concatenate(heads_out, axis=1).astype(jnp.bfloat16)
        att[...] = attended.reshape(att.shape)
        attr[t] = att[t]
        for s in range(1, tpn):
            copy_att(s).start()

    load_g.wait()
    load_u.wait()
    load_d.wait()

    def step(i, carry):
        @pl.when(i == n - 2)
        def _():
            for s in range(1, half):
                kv_far_in(s).wait_recv()
                kv_mate(s).start()

        @pl.when(i == n)
        def _():
            attention()

        @pl.when(i < n)
        def _():
            s = lax.rem(i + half, n)

            @pl.when(s > 0)
            def _():
                copy_a(s).wait_recv()

                @pl.when(s >= half)
                def _():
                    copy_bx(s, t).start()

                copy_bc(s, t).start()

        @pl.when((i >= 1) & (i <= n))
        def _():
            s = lax.rem(i - 1 + half, n)

            @pl.when(s > 0)
            def _():
                copy_bx(s, peer).wait_recv()
                copy_c(s, peer).start()

        @pl.when((i >= 2) & (i <= n + 1))
        def _():
            s = lax.rem(i - 2 + half, n)
            src = source(s)

            @pl.when(s > 0)
            def _():
                copy_bc(s, partner).wait_recv()
                copy_c(s, opp).wait_recv()

            block = recv[src].astype(jnp.float32)
            count = block.shape[0] * cap
            lo = block[:, :cap].reshape(count, wide).astype(jnp.bfloat16)
            hi = block[:, cap:].reshape(count, wide).astype(jnp.bfloat16)
            gate = jnp.dot(lo, wgv[0:wide, :], preferred_element_type=jnp.float32) + jnp.dot(
                hi, wgv[wide:, :], preferred_element_type=jnp.float32
            )
            upper = jnp.dot(lo, wuv[0:wide, :], preferred_element_type=jnp.float32) + jnp.dot(
                hi, wuv[wide:, :], preferred_element_type=jnp.float32
            )
            hidden = (gate / (1.0 + jnp.exp(-gate)) * upper).astype(jnp.bfloat16)
            down = jnp.dot(hidden, wdv[...], preferred_element_type=jnp.float32)
            shape = (tpn, cap, wide)
            part[src] = jnp.concatenate(
                [down[:, :wide].reshape(shape), down[:, wide:].reshape(shape)], axis=1
            ).astype(jnp.bfloat16)
            copy_r1(s, 1, opp).start()
            copy_r1(s, 0, partner).start()

        @pl.when((i >= 3) & (i <= n + 2))
        def _():
            s = lax.rem(i - 3 + half, n)
            src = source(s)
            copy_r1(s, 1, opp).wait_recv()
            copy_r1(s, 0, partner).wait_recv()
            s2[src] = (
                part[src, peer].astype(jnp.float32) + r1[src, 1].astype(jnp.float32)
            ).astype(jnp.bfloat16)
            copy_r2(s).start()

        @pl.when(i >= 4)
        def _():
            s = lax.rem(i - 4 + half, n)
            src = source(s)
            copy_r2(s).wait_recv()
            s3[src] = (
                part[src, t].astype(jnp.float32)
                + r1[src, 0].astype(jnp.float32)
                + r2[src].astype(jnp.float32)
            ).astype(jnp.bfloat16)

            @pl.when(s > 0)
            def _():
                copy_r3(s).start()

            @pl.when(s == 0)
            def _():
                rbuf[e] = s3[e]

        return carry

    lax.fori_loop(0, n + 4, step, 0)

    for s in range(1, tpn):
        copy_att_in(s).wait_recv()
    load_o.wait()
    joined = jnp.concatenate([attr[j] for j in range(tpn)], axis=1)
    mixed_ref[...] = jnp.dot(joined, owv[...], preferred_element_type=jnp.float32).astype(
        jnp.bfloat16
    )

    for s in range(1, n):
        copy_r3_in(s).wait_recv()
    picked = jnp.dot(
        sel[...], rbuf[...].reshape(lanes, wide), preferred_element_type=jnp.float32
    )
    load_w.wait()
    rw = [column(rw_ref[k : k + 1, :], 0) for k in range(top)]
    for h in range(2):
        acc = jnp.zeros((own_rows, wide), jnp.float32)
        for k in range(top):
            at = (2 * k + h) * own_rows
            acc = acc + rw[k] * picked[at : at + own_rows]
        out_ref[:, h * wide : (h + 1) * wide] = acc.astype(jnp.bfloat16)

    for s in range(1, half):
        kv_far(s).wait_send()
    for s in range(half):
        kv_mate(s).wait_send()
    for s in range(1, tpn):
        copy_att(s).wait_send()

    def drain(s, carry):
        copy_r1(s, 0, partner).wait_send()
        copy_r1(s, 1, opp).wait_send()
        copy_r2(s).wait_send()

        @pl.when(s > 0)
        def _():
            send_a(s).wait_send()
            copy_bx(s, t).wait_send()
            copy_bc(s, t).wait_send()
            copy_c(s, peer).wait_send()
            copy_r3(s).wait_send()

        return carry

    lax.fori_loop(0, n, drain, 0)


def fused_body(
    n,
    tpn,
    queries,
    key_cache,
    value_cache,
    cum_gate,
    out_weight,
    routed_input,
    norm_gain,
    routes,
    route_weight,
    expert_gate,
    expert_up,
    expert_down,
):
    seq = queries.shape[0]
    head = key_cache.shape[1]
    width = routed_input.shape[1]
    wide = width // 2
    own_rows = routed_input.shape[0] // tpn
    top = routes.shape[1]
    units = expert_gate.shape[2]
    cap = block_capacity(own_rows, top, n * expert_gate.shape[0])
    bf16 = jnp.bfloat16
    chunk = (2 * cap, wide)
    vmem = pl.BlockSpec(memory_space=pltpu.VMEM)
    anywhere = pl.BlockSpec(memory_space=pltpu.HBM)
    dma = pltpu.SemaphoreType.DMA
    mixed, out = pl.pallas_call(
        functools.partial(fused_kernel, n, tpn, cap),
        out_shape=(
            jax.ShapeDtypeStruct((seq // tpn, width), bf16),
            jax.ShapeDtypeStruct((own_rows, width), bf16),
        ),
        in_specs=[anywhere] * 12,
        out_specs=(vmem, vmem),
        scratch_shapes=[
            pltpu.VMEM(queries.shape, bf16),
            pltpu.VMEM(cum_gate.shape, jnp.float32),
            pltpu.VMEM((width // 128, 128), bf16),
            pltpu.VMEM((top, tpn * own_rows), jnp.int32),
            pltpu.VMEM((top, tpn * own_rows), jnp.float32),
            pltpu.VMEM((tpn, own_rows, width), bf16),
            pltpu.VMEM((width, units), bf16),
            pltpu.VMEM((width, units), bf16),
            pltpu.VMEM((units, width), bf16),
            pltpu.VMEM(out_weight.shape, bf16),
            pltpu.VMEM((n, 2 * head, seq), bf16),
            pltpu.VMEM((tpn, seq // tpn, queries.shape[1]), bf16),
            pltpu.VMEM((tpn, seq // tpn, queries.shape[1]), bf16),
            pltpu.VMEM((2 * top * own_rows, 2 * n * cap), bf16),
            pltpu.VMEM((n,) + chunk, bf16),
            pltpu.VMEM((n,) + chunk, bf16),
            pltpu.VMEM((n, tpn) + chunk, bf16),
            pltpu.VMEM((n, tpn) + chunk, bf16),
            pltpu.VMEM((n, 2) + chunk, bf16),
            pltpu.VMEM((n,) + chunk, bf16),
            pltpu.VMEM((n,) + chunk, bf16),
            pltpu.VMEM((n,) + chunk, bf16),
            pltpu.VMEM((n,) + chunk, bf16),
            dma((12 + tpn,)),
            dma((n,)),
            dma((n,)),
            dma((tpn,)),
            dma((tpn,)),
        ]
        + [dma((n,))] * 8
        + [dma((n, 2))] * 2
        + [dma((n,))] * 4,
        compiler_params=pltpu.CompilerParams(
            collective_id=0, has_side_effects=True, vmem_limit_bytes=60 * 1024 * 1024
        ),
    )(
        queries,
        cum_gate,
        norm_gain.reshape(width // 128, 128),
        routes.T,
        route_weight.T,
        key_cache,
        value_cache,
        out_weight,
        routed_input,
        expert_gate,
        expert_up,
        expert_down,
    )
    return mixed, out


def block_capacity(own_rows, top_count, expert_count):
    return max(2, own_rows * top_count * 3 // (2 * expert_count))


def slot_chooser(route_rows, expert_count, capacity):
    token_rows, top_count = route_rows.shape
    flat = route_rows.reshape(token_rows * top_count)
    same = (flat[:, None] == jnp.arange(expert_count, dtype=jnp.int32)[None, :]).astype(jnp.int32)
    earlier = jnp.cumsum(same, axis=0) - same
    rank = jnp.sum(earlier * same, axis=1)
    slot = flat * capacity + rank
    chosen = slot[:, None] == jnp.arange(expert_count * capacity, dtype=jnp.int32)[None, :]
    return chosen.astype(jnp.bfloat16).reshape(token_rows, top_count, expert_count * capacity)


def rms_rows(source, norm_gain):
    widened = source.astype(jnp.float32)
    scale = lax.rsqrt(jnp.mean(widened * widened, axis=-1, keepdims=True) + 1e-06)
    return (widened * scale * norm_gain.astype(jnp.float32)).astype(jnp.bfloat16)


def mixer_half(queries, key_cache, value_cache, cum_gate, out_weight):
    seq_rows = queries.shape[0]
    local_heads = key_cache.shape[0]
    head_size = key_cache.shape[1]
    group = queries.shape[1] // (local_heads * head_size)
    own_start = lax.axis_index("ep") * seq_rows
    query_heads = queries.reshape(seq_rows, local_heads, group, head_size)
    query_pos = own_start + jnp.arange(seq_rows, dtype=jnp.int32)
    gate_query = lax.dynamic_slice_in_dim(cum_gate, own_start, seq_rows, 1)
    gate_rows = jnp.transpose(gate_query)[:, :, None, None]
    scale = head_size ** (-0.5)
    best_start = jnp.full((seq_rows, local_heads, group), -jnp.inf, jnp.float32)
    total_start = jnp.zeros((seq_rows, local_heads, group), jnp.float32)
    summed_start = jnp.zeros((seq_rows, local_heads * group * head_size), jnp.float32)
    pieces = (
        lax.all_gather(key_cache, "ep", axis=2, tiled=True),
        lax.all_gather(value_cache, "ep", axis=2, tiled=True),
    )

    def update(state):
        best, total, summed = state
        key_piece, value_piece = pieces
        width = key_piece.shape[2]
        scores = (
            jnp.einsum("thgd,hds->thgs", query_heads, key_piece, preferred_element_type=jnp.float32)
            * scale
        )
        scores = scores + gate_rows - cum_gate[None, :, None, :]
        key_pos = jnp.arange(width, dtype=jnp.int32)
        allowed = key_pos[None, :] <= query_pos[:, None]
        scores = jnp.where(allowed[:, None, None, :], scores, -jnp.inf)
        new_best = jnp.max(scores, axis=-1)
        factor = jnp.exp(best - new_best)
        weights = jnp.exp(scores - new_best[..., None])
        new_total = total * factor + jnp.sum(weights, axis=-1)
        product = jnp.einsum(
            "thgs,hds->thgd",
            weights.astype(jnp.bfloat16),
            value_piece,
            preferred_element_type=jnp.float32,
        )
        new_summed = summed.reshape(product.shape) * factor[..., None] + product
        return (new_best, new_total, new_summed.reshape(seq_rows, local_heads * group * head_size))

    best, total, summed = lax.cond(
        jnp.int32(0) <= own_start,
        update,
        lambda state: state,
        (best_start, total_start, summed_start),
    )
    attended = summed.reshape(seq_rows, local_heads, group, head_size) / total[..., None]
    attended = attended.astype(jnp.bfloat16).reshape(seq_rows, local_heads * group * head_size)
    by_position = lax.all_to_all(attended, "tp", split_axis=0, concat_axis=1, tiled=True)
    return jnp.dot(by_position, out_weight, preferred_element_type=jnp.float32).astype(jnp.bfloat16)


def expert_half(routed_input, norm_gain, routes, route_weight, expert_gate, expert_up, expert_down):
    group_size = lax.axis_size("tp")
    ep_size = lax.axis_size("ep")
    tp_index = lax.axis_index("tp")
    seq_rows, width = routed_input.shape
    own_rows = seq_rows // group_size
    local_experts = expert_gate.shape[0]
    expert_count = local_experts * ep_size
    top_count = routes.shape[1]
    capacity = max(2, own_rows * top_count * 3 // (2 * expert_count))
    per_device = local_experts * capacity
    mine = lax.dynamic_slice_in_dim(routed_input, tp_index * own_rows, own_rows, 0)
    own_routes = lax.dynamic_slice_in_dim(routes, tp_index * own_rows, own_rows, 0)
    chooser = slot_chooser(own_routes, expert_count, capacity)
    normed = rms_rows(mine, norm_gain)
    outgoing = jnp.einsum("tks,td->sd", chooser, normed, preferred_element_type=jnp.float32).astype(
        jnp.bfloat16
    )
    arrived = lax.all_to_all(
        outgoing.reshape(1, ep_size, per_device, width),
        "ep",
        split_axis=1,
        concat_axis=1,
        tiled=True,
    )
    received = lax.all_gather(arrived, "tp", axis=0, tiled=True)
    blocks = received.shape[0]
    divide_point = received.reshape(blocks, ep_size, local_experts, capacity, width)
    gate = jnp.einsum(
        "abecd,edf->abecf", divide_point, expert_gate, preferred_element_type=jnp.float32
    )
    upper = jnp.einsum(
        "abecd,edf->abecf", divide_point, expert_up, preferred_element_type=jnp.float32
    )
    hidden = (jax.nn.silu(gate) * upper).astype(jnp.bfloat16)
    partial_value = jnp.einsum(
        "abecf,efd->abecd", hidden, expert_down, preferred_element_type=jnp.float32
    )
    rounded = lax.optimization_barrier(partial_value.astype(jnp.bfloat16)).astype(jnp.float32)
    summed = lax.psum_scatter(
        rounded.reshape(lax.axis_size("tp") * 1, ep_size, per_device, width).astype(jnp.bfloat16),
        "tp",
        scatter_dimension=0,
        tiled=True,
    )
    returned = lax.all_to_all(summed, "ep", split_axis=1, concat_axis=1, tiled=True)
    picked = jnp.einsum(
        "tks,sd->tkd",
        chooser,
        returned.reshape(ep_size * per_device, width),
        preferred_element_type=jnp.float32,
    )
    own_weight = lax.dynamic_slice_in_dim(route_weight, tp_index * own_rows, own_rows, 0)
    return jnp.sum(own_weight[:, :, None] * picked, axis=1).astype(jnp.bfloat16)


def body(
    queries,
    key_cache,
    value_cache,
    cum_gate,
    out_weight,
    routed_input,
    norm_gain,
    routes,
    route_weight,
    expert_gate,
    expert_up,
    expert_down,
):
    mixed_out = mixer_half(queries, key_cache, value_cache, cum_gate, out_weight)
    expert_out = expert_half(
        routed_input, norm_gain, routes, route_weight, expert_gate, expert_up, expert_down
    )
    return (mixed_out, expert_out)


def pick_body(
    n,
    tpn,
    queries,
    key_cache,
    value_cache,
    cum_gate,
    out_weight,
    routed_input,
    norm_gain,
    routes,
    route_weight,
    expert_gate,
    *rest,
):
    seq, columns = queries.shape
    own_rows = routed_input.shape[0] // tpn
    cap = block_capacity(own_rows, routes.shape[1], n * expert_gate.shape[0])
    fits = (
        tpn == 4
        and n >= 4
        and n & (n - 1) == 0
        and cap % 8 == 0
        and expert_gate.shape[0] == 1
        and key_cache.shape[0] == 1
        and seq % 128 == 0
    )
    args = (
        queries,
        key_cache,
        value_cache,
        cum_gate,
        out_weight,
        routed_input,
        norm_gain,
        routes,
        route_weight,
        expert_gate,
    ) + rest
    return fused_body(n, tpn, *args) if fits else body(*args)


def solution(mesh):
    return jax.shard_map(
        functools.partial(pick_body, mesh.shape["ep"], mesh.shape["tp"]),
        mesh=mesh,
        in_specs=(
            P("ep", "tp"),
            P("tp", None, "ep"),
            P("tp", None, "ep"),
            P("tp", None),
            P(),
            P("ep", None),
            P(),
            P("ep", None),
            P("ep", None),
            P("ep", None, "tp"),
            P("ep", None, "tp"),
            P("ep", "tp", None),
        ),
        out_specs=(P(("ep", "tp"), None), P(("ep", "tp"), None)),
        check_vma=False,
    )
```

```python
import functools

import jax
import jax.numpy as jnp
from jax import lax
from jax.experimental import pallas as pl
from jax.experimental.pallas import tpu as pltpu
from jax.sharding import PartitionSpec as P

MESH = pl.DeviceIdType.MESH


def fused_kernel(
    n,
    tpn,
    cap,
    q_any,
    gate_any,
    gain_any,
    routes_any,
    rw_any,
    k_any,
    v_any,
    ow_any,
    x_any,
    wg_any,
    wu_any,
    wd_any,
    mixed_ref,
    out_ref,
    q_ref,
    gate_ref,
    gain_ref,
    routes_ref,
    rw_ref,
    xbuf,
    wgv,
    wuv,
    wdv,
    owv,
    kv,
    att,
    attr,
    sel,
    sbuf,
    sbuf2,
    recv,
    part,
    r1,
    s2,
    r2,
    s3,
    rbuf,
    lsem,
    kvs,
    kvr,
    ats,
    atr,
    a_s,
    a_r,
    bx_s,
    bx_r,
    bc_s,
    bc_r,
    c_s,
    c_r,
    r1_s,
    r1_r,
    r2_s,
    r2_r,
    r3_s,
    r3_r,
):
    e = lax.axis_index("ep")
    t = lax.axis_index("tp")
    partner = t + 1 - 2 * lax.rem(t, 2)
    peer = lax.rem(t + 2, tpn)
    opp = lax.rem(partner + 2, tpn)
    mate = e + 1 - 2 * lax.rem(e, 2)
    half = n // 2
    _, own_rows, width = xbuf.shape
    wide = width // 2
    head = k_any.shape[1]
    seq = q_ref.shape[0]

    barrier = pltpu.get_barrier_semaphore()
    for s in range(1, n):
        pl.semaphore_signal(
            barrier, inc=1, device_id={"ep": lax.rem(e + s, n), "tp": t}, device_id_type=MESH
        )
    for s in range(1, tpn):
        pl.semaphore_signal(
            barrier, inc=1, device_id={"ep": e, "tp": lax.rem(t + s, tpn)}, device_id_type=MESH
        )

    def load_x(j):
        at = lax.rem(t + j, tpn) * own_rows
        return pltpu.make_async_copy(x_any.at[pl.ds(at, own_rows)], xbuf.at[j], lsem.at[12 + j])

    load_k = pltpu.make_async_copy(k_any.at[0], kv.at[e, pl.ds(0, head)], lsem.at[1])
    load_v = pltpu.make_async_copy(v_any.at[0], kv.at[e, pl.ds(head, head)], lsem.at[2])
    load_g = pltpu.make_async_copy(wg_any.at[0], wgv, lsem.at[3])
    load_u = pltpu.make_async_copy(wu_any.at[0], wuv, lsem.at[4])
    load_d = pltpu.make_async_copy(wd_any.at[0], wdv, lsem.at[5])
    load_o = pltpu.make_async_copy(ow_any, owv, lsem.at[6])
    load_q = pltpu.make_async_copy(q_any, q_ref, lsem.at[8])
    load_c = pltpu.make_async_copy(gate_any, gate_ref, lsem.at[9])
    load_n = pltpu.make_async_copy(gain_any, gain_ref, lsem.at[10])
    load_r = pltpu.make_async_copy(routes_any, routes_ref, lsem.at[11])
    load_w = pltpu.make_async_copy(rw_any, rw_ref, lsem.at[0])
    load_k.start()
    load_v.start()
    load_x(0).start()
    load_r.start()
    load_n.start()
    load_w.start()
    load_q.start()
    load_c.start()
    for j in range(1, tpn):
        load_x(j).start()
    load_g.start()
    load_u.start()
    load_d.start()
    load_o.start()

    def remote(src, dst, ssem, rsem, ep, tp):
        return pltpu.make_async_remote_copy(
            src_ref=src,
            dst_ref=dst,
            send_sem=ssem,
            recv_sem=rsem,
            device_id={"ep": ep, "tp": tp},
            device_id_type=MESH,
        )

    def kv_far(s):
        return remote(kv.at[e], kv.at[e], kvs.at[s], kvr.at[s], lax.rem(e + 2 * s, n), t)

    def kv_far_in(s):
        src = lax.rem(e - 2 * s + n, n)
        return remote(kv.at[src], kv.at[src], kvs.at[s], kvr.at[s], lax.rem(e + 2 * s, n), t)

    def kv_mate(s):
        src = lax.rem(e - 2 * s + n, n)
        return remote(kv.at[src], kv.at[src], kvs.at[half + s], kvr.at[half + s], mate, t)

    def kv_mate_in(s):
        src = lax.rem(mate - 2 * s + n, n)
        return remote(kv.at[src], kv.at[src], kvs.at[half + s], kvr.at[half + s], mate, t)

    def source(s):
        s = jnp.int32(s)
        flipped = jnp.int32(0)
        bit = 1
        while bit < n:
            ours = lax.rem(lax.div(e, jnp.int32(bit)), jnp.int32(2))
            theirs = lax.rem(lax.div(s, jnp.int32(bit)), jnp.int32(2))
            flipped = flipped + bit * (ours + theirs - 2 * ours * theirs)
            bit *= 2
        return flipped

    def send_a(s):
        dst = source(s)
        return remote(sbuf.at[dst], recv.at[e, t], a_s.at[s], a_r.at[s], dst, t)

    def send_near(s):
        dst = source(s)
        return remote(sbuf2.at[dst], recv.at[e, peer], bx_s.at[s], bx_r.at[s], dst, t)

    def copy_a(s):
        src = source(s)
        return remote(sbuf.at[src], recv.at[src, t], a_s.at[s], a_r.at[s], src, t)

    def copy_bx(s, col):
        src = source(s)
        return remote(recv.at[src, col], recv.at[src, col], bx_s.at[s], bx_r.at[s], e, peer)

    def copy_bc(s, col):
        src = source(s)
        return remote(recv.at[src, col], recv.at[src, col], bc_s.at[s], bc_r.at[s], e, partner)

    def copy_c(s, col):
        src = source(s)
        return remote(recv.at[src, col], recv.at[src, col], c_s.at[s], c_r.at[s], e, partner)

    def copy_r1(s, which, col):
        src = source(s)
        return remote(
            part.at[src, col], r1.at[src, which], r1_s.at[s, which], r1_r.at[s, which], e, partner
        )

    def copy_r2(s):
        src = source(s)
        return remote(s2.at[src], r2.at[src], r2_s.at[s], r2_r.at[s], e, peer)

    def copy_r3(s):
        src = source(s)
        return remote(s3.at[src], rbuf.at[e], r3_s.at[s], r3_r.at[s], src, t)

    def copy_r3_in(s):
        src = source(s)
        return remote(s3.at[src], rbuf.at[src], r3_s.at[s], r3_r.at[s], src, t)

    pl.semaphore_wait(barrier, n - 1 + tpn - 1)

    lanes = 2 * n * cap
    place = lax.broadcasted_iota(jnp.int32, (own_rows, lanes), 1).astype(jnp.float32) + 0.5
    expert = jnp.floor(place / (2.0 * cap))
    inside = place - 0.5 - expert * (2.0 * cap)
    right = inside >= cap
    slot = jnp.where(right, inside - cap, inside)
    top, share = routes_ref.shape

    def column(line, j):
        at = lax.rem(t + j, tpn) * own_rows
        own = lax.broadcasted_iota(jnp.int32, (own_rows, share), 1) == (
            lax.broadcasted_iota(jnp.int32, (own_rows, share), 0) + at
        )
        return jnp.sum(
            jnp.where(own, jnp.broadcast_to(line, own.shape), 0.0), axis=1, keepdims=True
        )

    def route(k, j):
        return column(routes_ref[k : k + 1, :].astype(jnp.float32), j)

    before = lax.broadcasted_iota(jnp.int32, (own_rows, own_rows), 1) < lax.broadcasted_iota(
        jnp.int32, (own_rows, own_rows), 0
    )

    def choose(j):
        named = [route(k, j) == expert for k in range(top)]
        total = sum([m.astype(jnp.float32) for m in named])
        rank = jnp.dot(
            before.astype(jnp.bfloat16),
            total.astype(jnp.bfloat16),
            preferred_element_type=jnp.float32,
        )
        hit = rank == slot
        chosen = jnp.where(hit, total, 0.0)
        spread = jnp.concatenate(
            [jnp.where(right, 0.0, chosen), jnp.where(right, chosen, 0.0)], axis=0
        )
        return spread.T.astype(jnp.bfloat16), hit, named

    load_r.wait()
    spread, hit, named = choose(0)
    load_n.wait()
    gain = gain_ref[...].astype(jnp.float32)
    gain = jnp.concatenate([gain[j : j + 1, :] for j in range(gain.shape[0])], axis=1)

    def halves(j):
        load_x(j).wait()
        x = xbuf[j].astype(jnp.float32)
        scale = lax.rsqrt(jnp.mean(x * x, axis=-1, keepdims=True) + 1e-06)
        normed = (x * scale * gain).astype(jnp.bfloat16)
        return jnp.concatenate([normed[:, :wide], normed[:, wide:]], axis=0)

    stacked = halves(0)
    outgoing = jnp.dot(spread, stacked, preferred_element_type=jnp.float32)
    sbuf[...] = outgoing.astype(jnp.bfloat16).reshape(sbuf.shape)
    for s in range(half, n):
        send_a(s).start()
    for s in range(1, half):
        send_a(s).start()
    keep = pltpu.make_async_copy(sbuf.at[e], recv.at[e, t], lsem.at[7])
    keep.start()
    outgoing = jnp.dot(choose(2)[0], halves(2), preferred_element_type=jnp.float32)
    sbuf2[...] = outgoing.astype(jnp.bfloat16).reshape(sbuf2.shape)
    for s in range(1, half):
        send_near(s).start()
    recv[e, peer] = sbuf2[e]
    keep.wait()
    for k in range(top):
        mine = jnp.where(hit & named[k], 1.0, 0.0)
        sel[2 * k * own_rows : (2 * k + 1) * own_rows, :] = jnp.where(right, 0.0, mine).astype(
            jnp.bfloat16
        )
        sel[(2 * k + 1) * own_rows : (2 * k + 2) * own_rows, :] = jnp.where(
            right, mine, 0.0
        ).astype(jnp.bfloat16)
    load_k.wait()
    load_v.wait()
    for s in range(1, half):
        kv_far(s).start()
    kv_mate(0).start()

    lane = lax.broadcasted_iota(jnp.int32, (own_rows, 2 * cap), 1)
    lane_right = lane >= cap
    lane_slot = jnp.where(lane_right, lane - cap, lane).astype(jnp.float32)
    mine_expert = e.astype(jnp.float32)
    for j in (1, 3):
        hits = sum(
            [jnp.where(route(k, j) == mine_expert, 1.0, 0.0) for k in range(top)]
        )
        hits = jnp.broadcast_to(hits, lane.shape)
        ranks = jnp.dot(
            before.astype(jnp.bfloat16),
            hits.astype(jnp.bfloat16),
            preferred_element_type=jnp.float32,
        )
        here = jnp.where(ranks == lane_slot, hits, 0.0)
        here = jnp.concatenate(
            [jnp.where(lane_right, 0.0, here), jnp.where(lane_right, here, 0.0)], axis=0
        )
        recv[e, lax.rem(t + j, tpn)] = jnp.dot(
            here.T.astype(jnp.bfloat16), halves(j), preferred_element_type=jnp.float32
        ).astype(jnp.bfloat16)

    def copy_att(s):
        dst = lax.rem(t + s, tpn)
        return remote(att.at[dst], attr.at[t], ats.at[s], atr.at[s], e, dst)

    def copy_att_in(s):
        src = lax.rem(t - s + tpn, tpn)
        return remote(att.at[src], attr.at[src], ats.at[s], atr.at[s], e, lax.rem(t + s, tpn))

    def attention():
        for s in range(half):
            kv_mate_in(s).wait_recv()
        load_q.wait()
        load_c.wait()
        own_gate = gate_ref[:, pl.ds(pl.multiple_of(e * seq, seq), seq)]
        eye = lax.broadcasted_iota(jnp.int32, (seq, seq), 0) == lax.broadcasted_iota(
            jnp.int32, (seq, seq), 1
        )
        gate_col = jnp.sum(
            jnp.where(eye, jnp.broadcast_to(own_gate, (seq, seq)), 0.0), axis=1, keepdims=True
        )
        key_pos = lax.broadcasted_iota(jnp.int32, (seq, n * seq), 1)
        query_pos = lax.broadcasted_iota(jnp.int32, (seq, n * seq), 0) + e * seq
        bias = gate_col - gate_ref[...]
        group = q_ref.shape[1] // head
        heads_out = []
        for g in range(group):
            q = q_ref[:, g * head : (g + 1) * head]
            scores = jnp.concatenate(
                [
                    jnp.dot(q, kv[j, 0:head, :], preferred_element_type=jnp.float32)
                    for j in range(n)
                ],
                axis=1,
            )
            scores = scores * (head ** (-0.5)) + bias
            scores = jnp.where(key_pos <= query_pos, scores, -jnp.inf)
            weights = jnp.exp(scores - jnp.max(scores, axis=-1, keepdims=True))
            whole = jnp.sum(weights, axis=-1, keepdims=True)
            weights = weights.astype(jnp.bfloat16)
            summed = jnp.zeros((seq, head), jnp.float32)
            for j in range(n):
                summed = summed + lax.dot_general(
                    weights[:, j * seq : (j + 1) * seq],
                    kv[j, head : 2 * head, :],
                    (((1,), (1,)), ((), ())),
                    preferred_element_type=jnp.float32,
                )
            heads_out.append(summed / whole)
        attended = jnp.concatenate(heads_out, axis=1).astype(jnp.bfloat16)
        att[...] = attended.reshape(att.shape)
        attr[t] = att[t]
        for s in range(1, tpn):
            copy_att(s).start()

    load_g.wait()
    load_u.wait()
    load_d.wait()

    def order(p):
        skip = lax.div(p, jnp.int32(half + 1))
        later = lax.div(p + n - 1, jnp.int32(n))
        return later * lax.rem(p + half - 1 + skip, n)

    def step(i, carry):
        @pl.when(i == n - 2)
        def _():
            for s in range(1, half):
                kv_far_in(s).wait_recv()
                kv_mate(s).start()

        @pl.when(i == n)
        def _():
            attention()

        @pl.when(i < n)
        def _():
            s = order(i)

            @pl.when(s > 0)
            def _():
                copy_a(s).wait_recv()

                @pl.when(s >= half)
                def _():
                    copy_bx(s, t).start()

                copy_bc(s, t).start()

        @pl.when((i >= 1) & (i <= n))
        def _():
            s = order(i - 1)

            @pl.when(s > 0)
            def _():
                copy_bx(s, peer).wait_recv()
                copy_c(s, peer).start()

        @pl.when((i >= 2) & (i <= n + 1))
        def _():
            s = order(i - 2)
            src = source(s)

            @pl.when(s > 0)
            def _():
                copy_bc(s, partner).wait_recv()
                copy_c(s, opp).wait_recv()

            block = recv[src].astype(jnp.float32)
            count = block.shape[0] * cap
            lo = block[:, :cap].reshape(count, wide).astype(jnp.bfloat16)
            hi = block[:, cap:].reshape(count, wide).astype(jnp.bfloat16)
            gate = jnp.dot(lo, wgv[0:wide, :], preferred_element_type=jnp.float32) + jnp.dot(
                hi, wgv[wide:, :], preferred_element_type=jnp.float32
            )
            upper = jnp.dot(lo, wuv[0:wide, :], preferred_element_type=jnp.float32) + jnp.dot(
                hi, wuv[wide:, :], preferred_element_type=jnp.float32
            )
            hidden = (gate / (1.0 + jnp.exp(-gate)) * upper).astype(jnp.bfloat16)
            down = jnp.dot(hidden, wdv[...], preferred_element_type=jnp.float32)
            shape = (tpn, cap, wide)
            part[src] = jnp.concatenate(
                [down[:, :wide].reshape(shape), down[:, wide:].reshape(shape)], axis=1
            ).astype(jnp.bfloat16)
            copy_r1(s, 1, opp).start()
            copy_r1(s, 0, partner).start()

        @pl.when((i >= 3) & (i <= n + 2))
        def _():
            s = order(i - 3)
            src = source(s)
            copy_r1(s, 1, opp).wait_recv()
            copy_r1(s, 0, partner).wait_recv()
            s2[src] = (
                part[src, peer].astype(jnp.float32) + r1[src, 1].astype(jnp.float32)
            ).astype(jnp.bfloat16)
            copy_r2(s).start()

        @pl.when(i >= 4)
        def _():
            s = order(i - 4)
            src = source(s)
            copy_r2(s).wait_recv()
            s3[src] = (
                part[src, t].astype(jnp.float32)
                + r1[src, 0].astype(jnp.float32)
                + r2[src].astype(jnp.float32)
            ).astype(jnp.bfloat16)

            @pl.when(s > 0)
            def _():
                copy_r3(s).start()

            @pl.when(s == 0)
            def _():
                rbuf[e] = s3[e]

        return carry

    lax.fori_loop(0, n + 4, step, 0)

    for s in range(1, tpn):
        copy_att_in(s).wait_recv()
    load_o.wait()
    joined = jnp.concatenate([attr[j] for j in range(tpn)], axis=1)
    mixed_ref[...] = jnp.dot(joined, owv[...], preferred_element_type=jnp.float32).astype(
        jnp.bfloat16
    )

    for s in range(1, n):
        copy_r3_in(s).wait_recv()
    picked = jnp.dot(
        sel[...], rbuf[...].reshape(lanes, wide), preferred_element_type=jnp.float32
    )
    load_w.wait()
    rw = [column(rw_ref[k : k + 1, :], 0) for k in range(top)]
    for h in range(2):
        acc = jnp.zeros((own_rows, wide), jnp.float32)
        for k in range(top):
            at = (2 * k + h) * own_rows
            acc = acc + rw[k] * picked[at : at + own_rows]
        out_ref[:, h * wide : (h + 1) * wide] = acc.astype(jnp.bfloat16)

    for s in range(1, half):
        kv_far(s).wait_send()
    for s in range(half):
        kv_mate(s).wait_send()
    for s in range(1, tpn):
        copy_att(s).wait_send()

    def drain(s, carry):
        copy_r1(s, 0, partner).wait_send()
        copy_r1(s, 1, opp).wait_send()
        copy_r2(s).wait_send()

        @pl.when(s > 0)
        def _():
            send_a(s).wait_send()
            copy_bx(s, t).wait_send()
            copy_bc(s, t).wait_send()
            copy_c(s, peer).wait_send()
            copy_r3(s).wait_send()

        return carry

    lax.fori_loop(0, n, drain, 0)


def fused_body(
    n,
    tpn,
    queries,
    key_cache,
    value_cache,
    cum_gate,
    out_weight,
    routed_input,
    norm_gain,
    routes,
    route_weight,
    expert_gate,
    expert_up,
    expert_down,
):
    seq = queries.shape[0]
    head = key_cache.shape[1]
    width = routed_input.shape[1]
    wide = width // 2
    own_rows = routed_input.shape[0] // tpn
    top = routes.shape[1]
    units = expert_gate.shape[2]
    cap = block_capacity(own_rows, top, n * expert_gate.shape[0])
    bf16 = jnp.bfloat16
    chunk = (2 * cap, wide)
    vmem = pl.BlockSpec(memory_space=pltpu.VMEM)
    anywhere = pl.BlockSpec(memory_space=pltpu.HBM)
    dma = pltpu.SemaphoreType.DMA
    mixed, out = pl.pallas_call(
        functools.partial(fused_kernel, n, tpn, cap),
        out_shape=(
            jax.ShapeDtypeStruct((seq // tpn, width), bf16),
            jax.ShapeDtypeStruct((own_rows, width), bf16),
        ),
        in_specs=[anywhere] * 12,
        out_specs=(vmem, vmem),
        scratch_shapes=[
            pltpu.VMEM(queries.shape, bf16),
            pltpu.VMEM(cum_gate.shape, jnp.float32),
            pltpu.VMEM((width // 128, 128), bf16),
            pltpu.VMEM((top, tpn * own_rows), jnp.int32),
            pltpu.VMEM((top, tpn * own_rows), jnp.float32),
            pltpu.VMEM((tpn, own_rows, width), bf16),
            pltpu.VMEM((width, units), bf16),
            pltpu.VMEM((width, units), bf16),
            pltpu.VMEM((units, width), bf16),
            pltpu.VMEM(out_weight.shape, bf16),
            pltpu.VMEM((n, 2 * head, seq), bf16),
            pltpu.VMEM((tpn, seq // tpn, queries.shape[1]), bf16),
            pltpu.VMEM((tpn, seq // tpn, queries.shape[1]), bf16),
            pltpu.VMEM((2 * top * own_rows, 2 * n * cap), bf16),
            pltpu.VMEM((n,) + chunk, bf16),
            pltpu.VMEM((n,) + chunk, bf16),
            pltpu.VMEM((n, tpn) + chunk, bf16),
            pltpu.VMEM((n, tpn) + chunk, bf16),
            pltpu.VMEM((n, 2) + chunk, bf16),
            pltpu.VMEM((n,) + chunk, bf16),
            pltpu.VMEM((n,) + chunk, bf16),
            pltpu.VMEM((n,) + chunk, bf16),
            pltpu.VMEM((n,) + chunk, bf16),
            dma((12 + tpn,)),
            dma((n,)),
            dma((n,)),
            dma((tpn,)),
            dma((tpn,)),
        ]
        + [dma((n,))] * 8
        + [dma((n, 2))] * 2
        + [dma((n,))] * 4,
        compiler_params=pltpu.CompilerParams(
            collective_id=0, has_side_effects=True, vmem_limit_bytes=60 * 1024 * 1024
        ),
    )(
        queries,
        cum_gate,
        norm_gain.reshape(width // 128, 128),
        routes.T,
        route_weight.T,
        key_cache,
        value_cache,
        out_weight,
        routed_input,
        expert_gate,
        expert_up,
        expert_down,
    )
    return mixed, out


def block_capacity(own_rows, top_count, expert_count):
    return max(2, own_rows * top_count * 3 // (2 * expert_count))


def slot_chooser(route_rows, expert_count, capacity):
    token_rows, top_count = route_rows.shape
    flat = route_rows.reshape(token_rows * top_count)
    same = (flat[:, None] == jnp.arange(expert_count, dtype=jnp.int32)[None, :]).astype(jnp.int32)
    earlier = jnp.cumsum(same, axis=0) - same
    rank = jnp.sum(earlier * same, axis=1)
    slot = flat * capacity + rank
    chosen = slot[:, None] == jnp.arange(expert_count * capacity, dtype=jnp.int32)[None, :]
    return chosen.astype(jnp.bfloat16).reshape(token_rows, top_count, expert_count * capacity)


def rms_rows(source, norm_gain):
    widened = source.astype(jnp.float32)
    scale = lax.rsqrt(jnp.mean(widened * widened, axis=-1, keepdims=True) + 1e-06)
    return (widened * scale * norm_gain.astype(jnp.float32)).astype(jnp.bfloat16)


def mixer_half(queries, key_cache, value_cache, cum_gate, out_weight):
    seq_rows = queries.shape[0]
    local_heads = key_cache.shape[0]
    head_size = key_cache.shape[1]
    group = queries.shape[1] // (local_heads * head_size)
    own_start = lax.axis_index("ep") * seq_rows
    query_heads = queries.reshape(seq_rows, local_heads, group, head_size)
    query_pos = own_start + jnp.arange(seq_rows, dtype=jnp.int32)
    gate_query = lax.dynamic_slice_in_dim(cum_gate, own_start, seq_rows, 1)
    gate_rows = jnp.transpose(gate_query)[:, :, None, None]
    scale = head_size ** (-0.5)
    best_start = jnp.full((seq_rows, local_heads, group), -jnp.inf, jnp.float32)
    total_start = jnp.zeros((seq_rows, local_heads, group), jnp.float32)
    summed_start = jnp.zeros((seq_rows, local_heads * group * head_size), jnp.float32)
    pieces = (
        lax.all_gather(key_cache, "ep", axis=2, tiled=True),
        lax.all_gather(value_cache, "ep", axis=2, tiled=True),
    )

    def update(state):
        best, total, summed = state
        key_piece, value_piece = pieces
        width = key_piece.shape[2]
        scores = (
            jnp.einsum("thgd,hds->thgs", query_heads, key_piece, preferred_element_type=jnp.float32)
            * scale
        )
        scores = scores + gate_rows - cum_gate[None, :, None, :]
        key_pos = jnp.arange(width, dtype=jnp.int32)
        allowed = key_pos[None, :] <= query_pos[:, None]
        scores = jnp.where(allowed[:, None, None, :], scores, -jnp.inf)
        new_best = jnp.max(scores, axis=-1)
        factor = jnp.exp(best - new_best)
        weights = jnp.exp(scores - new_best[..., None])
        new_total = total * factor + jnp.sum(weights, axis=-1)
        product = jnp.einsum(
            "thgs,hds->thgd",
            weights.astype(jnp.bfloat16),
            value_piece,
            preferred_element_type=jnp.float32,
        )
        new_summed = summed.reshape(product.shape) * factor[..., None] + product
        return (new_best, new_total, new_summed.reshape(seq_rows, local_heads * group * head_size))

    best, total, summed = lax.cond(
        jnp.int32(0) <= own_start,
        update,
        lambda state: state,
        (best_start, total_start, summed_start),
    )
    attended = summed.reshape(seq_rows, local_heads, group, head_size) / total[..., None]
    attended = attended.astype(jnp.bfloat16).reshape(seq_rows, local_heads * group * head_size)
    by_position = lax.all_to_all(attended, "tp", split_axis=0, concat_axis=1, tiled=True)
    return jnp.dot(by_position, out_weight, preferred_element_type=jnp.float32).astype(jnp.bfloat16)


def expert_half(routed_input, norm_gain, routes, route_weight, expert_gate, expert_up, expert_down):
    group_size = lax.axis_size("tp")
    ep_size = lax.axis_size("ep")
    tp_index = lax.axis_index("tp")
    seq_rows, width = routed_input.shape
    own_rows = seq_rows // group_size
    local_experts = expert_gate.shape[0]
    expert_count = local_experts * ep_size
    top_count = routes.shape[1]
    capacity = max(2, own_rows * top_count * 3 // (2 * expert_count))
    per_device = local_experts * capacity
    mine = lax.dynamic_slice_in_dim(routed_input, tp_index * own_rows, own_rows, 0)
    own_routes = lax.dynamic_slice_in_dim(routes, tp_index * own_rows, own_rows, 0)
    chooser = slot_chooser(own_routes, expert_count, capacity)
    normed = rms_rows(mine, norm_gain)
    outgoing = jnp.einsum("tks,td->sd", chooser, normed, preferred_element_type=jnp.float32).astype(
        jnp.bfloat16
    )
    arrived = lax.all_to_all(
        outgoing.reshape(1, ep_size, per_device, width),
        "ep",
        split_axis=1,
        concat_axis=1,
        tiled=True,
    )
    received = lax.all_gather(arrived, "tp", axis=0, tiled=True)
    blocks = received.shape[0]
    divide_point = received.reshape(blocks, ep_size, local_experts, capacity, width)
    gate = jnp.einsum(
        "abecd,edf->abecf", divide_point, expert_gate, preferred_element_type=jnp.float32
    )
    upper = jnp.einsum(
        "abecd,edf->abecf", divide_point, expert_up, preferred_element_type=jnp.float32
    )
    hidden = (jax.nn.silu(gate) * upper).astype(jnp.bfloat16)
    partial_value = jnp.einsum(
        "abecf,efd->abecd", hidden, expert_down, preferred_element_type=jnp.float32
    )
    rounded = lax.optimization_barrier(partial_value.astype(jnp.bfloat16)).astype(jnp.float32)
    summed = lax.psum_scatter(
        rounded.reshape(lax.axis_size("tp") * 1, ep_size, per_device, width).astype(jnp.bfloat16),
        "tp",
        scatter_dimension=0,
        tiled=True,
    )
    returned = lax.all_to_all(summed, "ep", split_axis=1, concat_axis=1, tiled=True)
    picked = jnp.einsum(
        "tks,sd->tkd",
        chooser,
        returned.reshape(ep_size * per_device, width),
        preferred_element_type=jnp.float32,
    )
    own_weight = lax.dynamic_slice_in_dim(route_weight, tp_index * own_rows, own_rows, 0)
    return jnp.sum(own_weight[:, :, None] * picked, axis=1).astype(jnp.bfloat16)


def body(
    queries,
    key_cache,
    value_cache,
    cum_gate,
    out_weight,
    routed_input,
    norm_gain,
    routes,
    route_weight,
    expert_gate,
    expert_up,
    expert_down,
):
    mixed_out = mixer_half(queries, key_cache, value_cache, cum_gate, out_weight)
    expert_out = expert_half(
        routed_input, norm_gain, routes, route_weight, expert_gate, expert_up, expert_down
    )
    return (mixed_out, expert_out)


def pick_body(
    n,
    tpn,
    queries,
    key_cache,
    value_cache,
    cum_gate,
    out_weight,
    routed_input,
    norm_gain,
    routes,
    route_weight,
    expert_gate,
    *rest,
):
    seq, columns = queries.shape
    own_rows = routed_input.shape[0] // tpn
    cap = block_capacity(own_rows, routes.shape[1], n * expert_gate.shape[0])
    fits = (
        tpn == 4
        and n >= 4
        and n & (n - 1) == 0
        and cap % 8 == 0
        and expert_gate.shape[0] == 1
        and key_cache.shape[0] == 1
        and seq % 128 == 0
    )
    args = (
        queries,
        key_cache,
        value_cache,
        cum_gate,
        out_weight,
        routed_input,
        norm_gain,
        routes,
        route_weight,
        expert_gate,
    ) + rest
    return fused_body(n, tpn, *args) if fits else body(*args)


def solution(mesh):
    return jax.shard_map(
        functools.partial(pick_body, mesh.shape["ep"], mesh.shape["tp"]),
        mesh=mesh,
        in_specs=(
            P("ep", "tp"),
            P("tp", None, "ep"),
            P("tp", None, "ep"),
            P("tp", None),
            P(),
            P("ep", None),
            P(),
            P("ep", None),
            P("ep", None),
            P("ep", None, "tp"),
            P("ep", None, "tp"),
            P("ep", "tp", None),
        ),
        out_specs=(P(("ep", "tp"), None), P(("ep", "tp"), None)),
        check_vma=False,
    )
```
